32 devices in a mesh: ep: 8 (over z, core), tp: 4 (over y, x).
Axes of the slice: x: 2, y: 2, z: 4, core: 2. Of those that a mesh axis runs over, the one named last changes fastest.
Arguments:
- tokens: bfloat16 [128, 4096], P('ep', 'tp'), may hold values from -40 to 40
- routes: int32 [128, 4], P('ep'), may hold values from 0 to 15, all different within a row; in each aligned block of 16 rows (0 to 15, 16 to 31, ...) at most 6 rows name the same one
- gates: float32 [128, 4], P('ep'), may hold values from 0.1 to 1
- pre_gain: bfloat16 [4096], P('tp'), may hold values from 0.099609375 to 1.8984375
- expert_gate: bfloat16 [16, 4096, 1024], P('ep', 'tp'), may hold values from -0.09375 to 0.09375
- expert_up: bfloat16 [16, 4096, 1024], P('ep', 'tp'), may hold values from -0.09375 to 0.09375
- expert_down: bfloat16 [16, 1024, 4096], P('ep', None, 'tp'), may hold values from -0.125 to 0.125
- shared_gate: bfloat16 [4096, 1024], P('tp'), may hold values from -0.09375 to 0.09375
- shared_up: bfloat16 [4096, 1024], P('tp'), may hold values from -0.09375 to 0.09375
- shared_down: bfloat16 [1024, 4096], P(None, 'tp'), may hold values from -0.125 to 0.125
- out_gain: bfloat16 [4096], P('tp'), may hold values from 0.099609375 to 1.8984375
Outputs:
- mixed: bfloat16 [128, 4096], P('ep', 'tp')
The draws below stay inside these ranges and needn't reach their ends.
Inputs may be any that keep to these rules, and one draw needn't show every extreme that they name: `routes`: each row names 4 different experts, and expert e is held by index e // 2 of ep. Among the 16 rows of one index of ep no expert is named by more than 6 rows, and in every draw some expert is named by exactly 6 rows of some index.
All inputs are finite; a program needn't handle non-finite values.
Results may differ from the reference program's by a relative error of at most 0.012.
Values may be sent and summed in bfloat16 or wider, within the bound.
A program may use at most 64 MiB of HBM per device.

```python
import math
import jax
import jax.numpy as jnp
import numpy as np
from jax import lax

D = 4096
FE = 1024
FS = 1024
TOP = 4
TOK_DEV = 16
EXPERTS = 16
CAP = 6
TOKENS = 128
N_EP = 8


def scaled_columns(key, shape, fan_in):
    first = jax.random.fold_in(key, 0)
    position = jnp.arange(shape[-1], dtype=jnp.float32) / shape[-1]
    base = jnp.clip(jax.random.normal(first, shape, jnp.float32), -4.0, 4.0)
    column = 10.0 ** (position - 1.0)
    return base * column * fan_in ** (-0.5)


def draw_expert_down(key, part):
    return scaled_columns(jax.random.fold_in(key, 11), (EXPERTS, FE, D), FE).astype(jnp.bfloat16)


def draw_shared_down(key, part):
    return scaled_columns(jax.random.fold_in(key, 12), (FS, D), FS).astype(jnp.bfloat16)


def draw_tokens(key, part):
    first, second = jax.random.split(jax.random.fold_in(key, 13), 2)
    position = jnp.arange(D, dtype=jnp.float32) / D
    row_scale = 10.0 ** jax.random.uniform(second, (TOKENS, 1), jnp.float32)
    base = jnp.clip(jax.random.normal(first, (TOKENS, D), jnp.float32), -4.0, 4.0)
    column = 10.0 ** position
    return (base * column * row_scale / 10.0).astype(jnp.bfloat16)


def shard_levels(own_key, shape, cuts, low, high):
    def one(dim, parts):
        heights = jax.random.uniform(jax.random.fold_in(jax.random.fold_in(own_key, 6), dim), (parts,), jnp.float32, low / len(cuts), high / len(cuts))
        return jnp.repeat(jnp.exp(heights), shape[dim] // parts).reshape((-1,) + (1,) * (len(shape) - dim - 1))

    level = one(*cuts[0])
    for cut in cuts[1:]:
        level = level * one(*cut)
    return level


def assign_block(key, own, number, rows, count, top, limit, slope):
    order = jax.random.permutation(key, count)
    crowded, ordinary = load_shares(count, rows * top, limit, slope, True), load_shares(count, rows * top, limit, slope, False)
    places = jnp.arange(count)

    def named(lengths, turn):
        used = int((lengths > 0).sum())
        fixed = max(1, used // 4)
        shifted = fixed + (places - fixed + turn * (used - fixed)) % max(1, count - fixed)
        return jnp.zeros((count,), jnp.int32).at[order[jnp.where(places < fixed, places, shifted)]].set(jnp.asarray(lengths, jnp.int32))

    lengths = jnp.where(number % 4 == 0, named(crowded, number // 4), named(ordinary, number - number // 4 - 1))
    mixed = jax.random.permutation(jax.random.fold_in(own, 3), count)
    giver, taker = mixed[0:count // 2 * 2:2], mixed[1:count // 2 * 2:2]
    margin = jnp.minimum(lengths[giver] - 1, limit - lengths[taker]) // 2
    margin = jnp.where((giver == order[0]) | (taker == order[0]) | (lengths[taker] == 0), 0, jnp.maximum(margin, 0))
    shifted = jax.random.randint(jax.random.fold_in(own, 4), (count // 2,), 0, 1 << 20) % (margin + 1)
    lengths = lengths.at[giver].add(-shifted).at[taker].add(shifted)
    members = jnp.searchsorted(jnp.cumsum(lengths), jnp.arange(rows * top), side="right").astype(jnp.int32)
    table = members.reshape(top, rows).T
    table = table[jax.random.permutation(jax.random.fold_in(own, 1), rows)]
    turn = jax.random.randint(jax.random.fold_in(own, 2), (rows, 1), 0, top)
    return jnp.take_along_axis(table, (jnp.arange(top)[None, :] + turn) % top, axis=1)


def load_shares(number_of, total, most, lean, full):
    loads = [(1 << 20) // math.isqrt(standing ** lean) + 1 for standing in range(1, number_of + 1)]
    largest = most if full else min(most, max(-(-total // number_of), total * loads[0] // sum(loads)))
    least = 1 if total - largest >= number_of - 1 else 0
    given, rest = [largest] + [least] * (number_of - 1), total - largest - least * (number_of - 1)
    while rest > 0:
        movable = [i for i in range(1, number_of) if given[i] < largest] or [i for i in range(1, number_of) if given[i] < most]
        pool, remaining = sum([loads[i] for i in movable]), rest
        for i in movable:
            extra = min(most - given[i], max(1, remaining * loads[i] // pool), rest)
            given[i] = given[i] + extra
            rest = rest - extra
    return np.array(given)


def normal_values(own_key, shape, width, most, pieces=(), held_as=jnp.bfloat16):
    array = jax.random.normal(own_key, shape, jnp.float32) * width
    if len(pieces) > 0:
        array = shard_levels(own_key, shape, pieces, -0.22, 0.18) * array
    return jnp.clip(array, min=-most, max=most).astype(held_as)


def setup_inputs(seed: int = 0) -> dict:
    key_list = jax.random.split(jax.random.key(seed), 12)
    tokens = draw_tokens(jax.random.fold_in(key_list[11], 71), 0)
    routes_keys = jax.random.split(jax.random.fold_in(key_list[1], 1), TOKENS // TOK_DEV)
    routes_turns = jax.random.permutation(jax.random.fold_in(key_list[1], 3), TOKENS // TOK_DEV)
    routes = jax.vmap(lambda own, number: assign_block(jax.random.fold_in(key_list[1], 2), own, number, TOK_DEV, EXPERTS, TOP, CAP, 2))(routes_keys, routes_turns).reshape((TOKENS, TOP))
    gates = jnp.clip(jnp.exp(math.log(1.0) - 2.3025851 * jax.random.uniform(key_list[2], (TOKENS, TOP), jnp.float32) ** shard_levels(key_list[2], (TOKENS, TOP), ((0, 8),), -0.2, 0.2)), 0.1, 1.0)
    pre_gain = jnp.clip(1.0 + 0.18 * jax.random.normal(key_list[3], (D,), jnp.float32), 0.099609375, 1.8984375).astype(jnp.bfloat16)
    expert_gate = normal_values(key_list[4], (EXPERTS, D, FE), D ** -0.5, 0.09375, ((0, 8), (1, 4)))
    expert_up = normal_values(key_list[5], (EXPERTS, D, FE), D ** -0.5, 0.09375, ((0, 8), (1, 4)))
    expert_down = draw_expert_down(jax.random.fold_in(key_list[11], 71), 0)
    shared_gate = normal_values(key_list[7], (D, FS), D ** -0.5, 0.09375, ((0, 4),))
    shared_up = normal_values(key_list[8], (D, FS), D ** -0.5, 0.09375, ((0, 4),))
    shared_down = draw_shared_down(jax.random.fold_in(key_list[11], 71), 0)
    out_gain = jnp.clip(1.0 + 0.18 * jax.random.normal(key_list[10], (D,), jnp.float32), 0.099609375, 1.8984375).astype(jnp.bfloat16)
    return dict(tokens=tokens, routes=routes, gates=gates, pre_gain=pre_gain, expert_gate=expert_gate, expert_up=expert_up, expert_down=expert_down, shared_gate=shared_gate, shared_up=shared_up, shared_down=shared_down, out_gain=out_gain)


def normalize(values, gain):
    as_float = values.astype(jnp.float32)
    scale = lax.rsqrt(lax.optimization_barrier(jnp.mean(as_float * as_float, axis=-1, keepdims=True)) + 1e-06)
    return as_float * scale * gain.astype(jnp.float32)

def reference(tokens, routes, gates, pre_gain, expert_gate, expert_up, expert_down, shared_gate, shared_up, shared_down, out_gain):
    normed = normalize(tokens, pre_gain).astype(jnp.bfloat16)
    labels = jnp.arange(EXPERTS, dtype=jnp.int32)
    picked = routes[:, :, None] == labels[None, None, :]
    onehot = lax.optimization_barrier(jnp.sum(picked.astype(jnp.int32), axis=1))
    dense_gate = lax.optimization_barrier(jnp.sum(jnp.where(picked, gates[:, :, None], jnp.zeros((), jnp.float32)), axis=1))
    blocked = onehot.reshape(N_EP, TOK_DEV, EXPERTS)
    slot_index = (jnp.cumsum(blocked, axis=1) - blocked).reshape(TOKENS, EXPERTS).astype(jnp.int32)
    block_of = jnp.arange(TOKENS, dtype=jnp.int32) // TOK_DEV
    target_row = jnp.where(onehot > 0, block_of[:, None] * CAP + slot_index, -1).astype(jnp.int32)
    row_index = jnp.arange(N_EP * CAP, dtype=jnp.int32)

    def per_expert(accumulated, expert_index):
        select = row_index[:, None] == target_row[:, expert_index][None, :]
        buffer = jnp.dot(select.astype(jnp.bfloat16), normed, preferred_element_type=jnp.float32).astype(jnp.bfloat16)
        gate_act = jnp.dot(buffer, expert_gate[expert_index], preferred_element_type=jnp.float32)
        up_act = jnp.dot(buffer, expert_up[expert_index], preferred_element_type=jnp.float32)
        hidden = (jax.nn.silu(gate_act) * up_act).astype(jnp.bfloat16)
        result = jnp.dot(hidden, expert_down[expert_index], preferred_element_type=jnp.float32).astype(jnp.bfloat16)
        weight = jnp.where(select, dense_gate[:, expert_index][None, :], jnp.zeros((), jnp.float32))
        accumulated = accumulated + jnp.dot(weight.T, result.astype(jnp.float32), precision=lax.Precision.HIGHEST)
        return (accumulated, None)
    routed, _ = lax.scan(per_expert, jnp.zeros((TOKENS, D), jnp.float32), jnp.arange(EXPERTS, dtype=jnp.int32))
    shared_gate_act = jnp.dot(normed, shared_gate, preferred_element_type=jnp.float32)
    shared_up_act = jnp.dot(normed, shared_up, preferred_element_type=jnp.float32)
    shared_hidden = (jax.nn.silu(shared_gate_act) * shared_up_act).astype(jnp.bfloat16)
    shared_out = jnp.dot(shared_hidden, shared_down, preferred_element_type=jnp.float32)
    combined = routed + shared_out
    return normalize(combined, out_gain).astype(jnp.bfloat16)
```

```python
import functools
import jax
import jax.numpy as jnp
from jax import lax
from jax.experimental import pallas as pl
from jax.experimental.pallas import tpu as pltpu
from jax.sharding import PartitionSpec as P

D = 4096


def normalize(values, gain, squares, width):
    scale = lax.rsqrt(squares[:, None] / width + 1e-06)
    return values * scale * gain.astype(jnp.float32)


def expert_apply(buffer, expert_gate, expert_up, expert_down, shared_gate_part, shared_up_part):
    gate_part = jnp.einsum(
        "secd,edf->secf", buffer, expert_gate, preferred_element_type=jnp.float32
    )
    up_part = jnp.einsum("secd,edf->secf", buffer, expert_up, preferred_element_type=jnp.float32)
    gate_act, up_act, shared_gate_act, shared_up_act = lax.psum(
        (gate_part, up_part, shared_gate_part, shared_up_part), "tp"
    )
    hidden = (jax.nn.silu(gate_act) * up_act).astype(jnp.bfloat16)
    shared_hidden = (jax.nn.silu(shared_gate_act) * shared_up_act).astype(jnp.bfloat16)
    results = jnp.einsum(
        "secf,efd->secd", hidden, expert_down, preferred_element_type=jnp.float32
    ).astype(jnp.bfloat16)
    return (results, shared_hidden)


def on_device(
    tokens,
    routes,
    gates,
    pre_gain,
    expert_gate,
    expert_up,
    expert_down,
    shared_gate,
    shared_up,
    shared_down,
    out_gain,
):
    own_rows = tokens.astype(jnp.float32)
    in_squares = lax.psum(jnp.sum(own_rows * own_rows, axis=1), "tp")
    normed = normalize(own_rows, pre_gain, in_squares, D).astype(jnp.bfloat16)
    shared_gate_part = jnp.dot(normed, shared_gate, preferred_element_type=jnp.float32)
    shared_up_part = jnp.dot(normed, shared_up, preferred_element_type=jnp.float32)
    tok_count = tokens.shape[0]
    top_count = routes.shape[1]
    groups = lax.axis_size("ep")
    local_experts = expert_gate.shape[0]
    experts_all = local_experts * groups
    capacity = max(2, 3 * tok_count * top_count // (2 * experts_all))
    places = jnp.arange(capacity, dtype=jnp.int32)
    zero_value = jnp.zeros((), jnp.float32)
    labels = jnp.arange(experts_all, dtype=jnp.int32)
    picked = routes[:, :, None] == labels[None, None, :]
    onehot = jnp.sum(picked.astype(jnp.int32), axis=1)
    dense_gate = jnp.sum(jnp.where(picked, gates[:, :, None], zero_value), axis=1)
    slot_index = jnp.cumsum(onehot, axis=0) - onehot
    select = (slot_index.T[:, None, :] == places[None, :, None]) & (onehot.T[:, None, :] > 0)
    outgoing = jnp.einsum(
        "ect,td->ecd", select.astype(jnp.bfloat16), normed, preferred_element_type=jnp.float32
    ).astype(jnp.bfloat16)
    outgoing = outgoing.reshape(groups, local_experts, capacity, normed.shape[1])
    received = lax.all_to_all(outgoing, "ep", split_axis=0, concat_axis=0, tiled=True)
    results, shared_hidden = expert_apply(
        received, expert_gate, expert_up, expert_down, shared_gate_part, shared_up_part
    )
    returned = lax.all_to_all(results, "ep", split_axis=0, concat_axis=0, tiled=True)
    weight = jnp.where(select, dense_gate.T[:, None, :], zero_value)
    returned_rows = returned.reshape(experts_all, capacity, normed.shape[1]).astype(jnp.float32)
    routed = jnp.einsum("ect,ecd->td", weight, returned_rows, precision=lax.Precision.HIGHEST)
    shared_out = jnp.dot(shared_hidden, shared_down, preferred_element_type=jnp.float32)
    combined = routed + shared_out
    out_squares = lax.psum(jnp.sum(combined * combined, axis=1), "tp")
    return normalize(combined, out_gain, out_squares, D).astype(jnp.bfloat16)


F32 = jnp.float32
BF16 = jnp.bfloat16
LANES = 128


def flip(index, mask):
    out, bit = index, 1
    while bit <= mask:
        if mask & bit:
            out = out + bit - 2 * bit * ((index // bit) % 2)
        bit *= 2
    return out


def iota(shape, dim):
    return lax.broadcasted_iota(jnp.int32, shape, dim)


def dot(a, b):
    return jnp.dot(a, b, preferred_element_type=F32)


def fused_kernel(
    n_ep, n_tp, cap, width,
    tok_hbm, routes_hbm, gates_hbm, pre_hbm, eg_hbm, eu_hbm, ed_hbm, sg_hbm, su_hbm, sd_hbm, outg_hbm,
    o_ref,
    tok_ref, routes_ref, gates_ref, pre_ref, outg_ref,
    wg, wu, wd, sg, su, sd,
    xall, ss_all, buf,
    rs_send, rs_recv, rs_own, rsh_send, rsh_recv, rsh_own,
    hid, hidsh, acc, yown, ysend, yhold, ypair, zsend, zrecv, sq_all,
    w_sem, x_send, x_recv, f_send, f_recv, ss_send, ss_recv, rs_ssem, rs_rsem, rsh_ssem, rsh_rsem,
    h_ssem, h_rsem, hs_ssem, hs_rsem, p_ssem, p_rsem, y_ssem, y_rsem, q_ssem, q_rsem,
):
    me = lax.axis_index("ep")
    mine = lax.axis_index("tp")
    tok, dim = tok_ref.shape
    local = eg_hbm.shape[0]
    experts = local * n_ep
    top = routes_hbm.shape[0]
    per = n_ep * cap
    rows = local * per
    hidden = eg_hbm.shape[2]
    part = hidden // n_tp
    total = n_ep * tok
    far = list(range(2, n_ep, 2))
    tp_masks = sorted(range(1, n_tp), key=lambda m: -bin(m).count("1"))
    pending = []

    def at_ep(mask):
        return {"ep": flip(me, mask)}

    def at_tp(mask):
        return {"tp": flip(mine, mask)}

    barrier = pltpu.get_barrier_semaphore()
    for m in far + [1]:
        pl.semaphore_signal(barrier, inc=1, device_id=at_ep(m), device_id_type=pl.DeviceIdType.MESH)
    for m in range(1, n_tp):
        pl.semaphore_signal(barrier, inc=1, device_id=at_tp(m), device_id_type=pl.DeviceIdType.MESH)

    copies = {}

    def fetch(name, src, dst, index):
        copies[name] = pltpu.make_async_copy(src, dst, w_sem.at[index])
        copies[name].start()

    small = 3 + 3 * local
    fetch("routes", routes_hbm, routes_ref, small)
    fetch("gates", gates_hbm, gates_ref, small + 1)
    fetch("tok", tok_hbm, tok_ref, small + 2)
    fetch("pre", pre_hbm, pre_ref, small + 3)
    fetch("outg", outg_hbm, outg_ref, small + 4)
    fetch("sg", sg_hbm, sg, 0)
    fetch("su", su_hbm, su, 1)
    for e in range(local):
        fetch(("g", e), eg_hbm.at[e], wg.at[e], 3 + e)
        fetch(("u", e), eu_hbm.at[e], wu.at[e], 3 + local + e)
    fetch("sd", sd_hbm, sd, 2)
    for e in range(local):
        fetch(("d", e), ed_hbm.at[e], wd.at[e], 3 + 2 * local + e)

    def send(src, dst, ssem, rsem, where):
        copy = pltpu.make_async_remote_copy(
            src_ref=src, dst_ref=dst, send_sem=ssem, recv_sem=rsem,
            device_id=where, device_id_type=pl.DeviceIdType.MESH,
        )
        copy.start()
        pending.append(copy)
        return copy

    def flat_gain(ref):
        value = ref[...].astype(F32)
        return jnp.concatenate([value[i : i + 1, :] for i in range(ref.shape[0])], axis=1)

    copies["routes"].wait()
    copies["gates"].wait()
    row = iota((LANES, tok), 0)
    names = row % experts
    dense = jnp.zeros((LANES, tok), F32)
    for k in range(top):
        dense = dense + jnp.where(routes_ref[k : k + 1, :] == names, gates_ref[k : k + 1, :], 0.0)
    earlier = jnp.where(iota((tok, tok), 0) < iota((tok, tok), 1), 1.0, 0.0).astype(BF16)
    slots = dot(jnp.where(dense > 0.0, 1.0, 0.0).astype(BF16), earlier)
    slots = jnp.where(dense > 0.0, slots + 1.0, 0.0)

    def terms(value):
        hi = value.astype(BF16).astype(F32)
        mid = (value - hi).astype(BF16).astype(F32)
        return hi, mid, value - hi - mid

    def choose(index, values):
        out = 0.0
        for i, value in enumerate(values):
            out = jnp.where(index == i, value, out)
        return out

    listed = choose(row // experts, terms(dense) + (slots,)).astype(BF16)
    eye = jnp.where(iota((tok, tok), 0) == iota((tok, tok), 1), 1.0, 0.0).astype(BF16)
    meta = lax.dot_general(eye, listed, (((1,), (1,)), ((), ())), preferred_element_type=F32)
    copies["tok"].wait()
    copies["pre"].wait()
    x = tok_ref[...].astype(F32)
    xall[me, :, :dim] = (x * flat_gain(pre_ref)).astype(BF16)
    squares = jnp.sum(x * x, axis=1, keepdims=True)
    lane = iota((tok, LANES), 1)
    meta = jnp.where(lane < 4 * experts, meta, choose(lane - 4 * experts, terms(squares)))
    xall[me, :, dim:] = meta.astype(BF16)

    pl.semaphore_wait(barrier, len(far) + 1 + n_tp - 1)

    own_block = xall.at[me]
    got = {}
    for m in far + [1]:
        got[m] = send(own_block, own_block, x_send.at[m], x_recv.at[m], at_ep(m))

    xs = xall[me, :, :dim]
    copies["sg"].wait()
    copies["su"].wait()
    shared_in = {}
    for m in tp_masks + [0]:
        cols = pl.ds(pl.multiple_of(flip(mine, m) * part, part), part)
        g = dot(xs, sg[:, cols])
        u = dot(xs, su[:, cols])
        if m:
            rsh_send[m - 1, :, :part] = g.astype(BF16)
            rsh_send[m - 1, :, part:] = u.astype(BF16)
            shared_in[m] = send(rsh_send.at[m - 1], rsh_recv.at[m - 1], rsh_ssem.at[m], rsh_rsem.at[m], at_tp(m))
        else:
            rsh_own[:, :part] = g
            rsh_own[:, part:] = u

    relayed = []
    for m in far:
        got[m].wait_recv()
        block = xall.at[flip(me, m)]
        relayed.append(send(block, block, f_send.at[m], f_recv.at[m], at_ep(1)))
    got[1].wait_recv()
    for copy in relayed:
        copy.wait_recv()

    tail = xall[:, :, dim:].reshape(total, LANES)
    row8, lane8 = iota((8, LANES), 0), iota((8, LANES), 1)
    gate_lane = lane8 < 3 * experts
    slot_lane = (lane8 >= 3 * experts) & (lane8 < 4 * experts)
    mine8 = me * local + row8
    pick = (
        ((row8 < local) & gate_lane & (lane8 % experts == mine8))
        | ((row8 == local) & (lane8 >= 4 * experts))
        | ((row8 > local) & (row8 <= 2 * local) & slot_lane & (lane8 % experts == mine8 - local - 1))
    )
    table = lax.dot_general(
        jnp.where(pick, 1.0, 0.0).astype(BF16), tail, (((1,), (1,)), ((), ())), preferred_element_type=F32
    )
    ss_all[mine] = table
    ss_in = [
        send(ss_all.at[mine], ss_all.at[mine], ss_send.at[m], ss_recv.at[m], at_tp(m)) for m in tp_masks
    ]
    first = (iota((8, total), 1) // tok) * cap - 1
    target = jnp.where(table > 0.5, first + table.astype(jnp.int32), -1)
    pieces = [
        jnp.where(iota((per, total), 0) == target[local + 1 + e : local + 2 + e, :], 1.0, 0.0)
        for e in range(local)
    ]
    gate_col = jnp.concatenate(
        [jnp.sum(pieces[e] * table[e : e + 1, :], axis=1, keepdims=True) for e in range(local)], axis=0
    )
    own = jnp.where(iota((tok, total), 1) == me * tok + iota((tok, total), 0), 1.0, 0.0)
    select = jnp.concatenate(pieces, axis=0)
    chosen = select.astype(BF16)
    flat = xall[:, :, :dim].reshape(total, dim)
    buf[...] = dot(chosen, flat).astype(BF16)

    routed_in = {}
    for e in range(local):
        copies["g", e].wait()
        copies["u", e].wait()
        here = pl.ds(e * per, per)
        rhs = buf[here, :]
        for m in tp_masks + [0]:
            cols = pl.ds(pl.multiple_of(flip(mine, m) * part, part), part)
            g = dot(rhs, wg[e, :, cols])
            u = dot(rhs, wu[e, :, cols])
            if m:
                rs_send[m - 1, here, :part] = g.astype(BF16)
                rs_send[m - 1, here, part:] = u.astype(BF16)
                routed_in[m, e] = send(
                    rs_send.at[m - 1, here], rs_recv.at[m - 1, here],
                    rs_ssem.at[m * local + e], rs_rsem.at[m * local + e], at_tp(m),
                )
            else:
                rs_own[here, :part] = g
                rs_own[here, part:] = u

    for copy in ss_in:
        copy.wait_recv()
    ss = ss_all[0, local : local + 1, :]
    for q in range(1, n_tp):
        ss = ss + ss_all[q, local : local + 1, :]
    scale = lax.rsqrt(ss / width + 1e-06)
    row_scale = jnp.sum(select * scale, axis=1, keepdims=True)
    own_scale = jnp.sum(own * scale, axis=1, keepdims=True)

    def activate(sums, by):
        g, u = sums[:, :part] * by, sums[:, part:] * by
        return (g / (1.0 + jnp.exp(-g)) * u).astype(BF16)

    routed_hid, shared_hid = {}, []
    for e in range(local):
        here = pl.ds(e * per, per)
        sums = rs_own[here, :]
        for m in tp_masks:
            routed_in[m, e].wait_recv()
            sums = sums + rs_recv[m - 1, here, :].astype(F32)
        hid[mine, here, :] = activate(sums, row_scale[e * per : (e + 1) * per, :])
        for m in tp_masks:
            block = hid.at[mine, here]
            routed_hid[m, e] = send(block, block, h_ssem.at[m * local + e], h_rsem.at[m * local + e], at_tp(m))
        if e == 0:
            sums = rsh_own[...]
            for m in tp_masks:
                shared_in[m].wait_recv()
                sums = sums + rsh_recv[m - 1].astype(F32)
            hidsh[mine] = activate(sums, own_scale)
            block = hidsh.at[mine]
            shared_hid = [send(block, block, hs_ssem.at[m], hs_rsem.at[m], at_tp(m)) for m in tp_masks]

    for e in range(local):
        copies["d", e].wait()

    def down(q, e):
        piece = pl.ds(pl.multiple_of(q * part, part), part)
        return dot(hid[q, pl.ds(e * per, per), :], wd[e, piece, :])

    for e in range(local):
        acc[pl.ds(e * per, per), :] = down(mine, e)
    copies["sd"].wait()
    for copy in shared_hid:
        copy.wait_recv()
    shared_out = dot(hidsh[0], sd[0:part, :])
    for q in range(1, n_tp):
        shared_out = shared_out + dot(hidsh[q], sd[q * part : (q + 1) * part, :])
    yown[...] = shared_out
    for e in range(local):
        for m in tp_masks[::-1]:
            routed_hid[m, e].wait_recv()
            acc[pl.ds(e * per, per), :] += down(flip(mine, m), e)

    gated = (acc[...] * gate_col).astype(BF16)
    back = lax.dot_general(chosen, gated, (((0,), (0,)), ((), ())), preferred_element_type=F32)
    back = back.reshape(n_ep, tok, dim)
    ysend[...] = back.astype(BF16)
    yhold[...] = back
    paired = {}
    for m in far + [0]:
        paired[m] = send(ysend.at[flip(me, m + 1)], ypair.at[m // 2], p_ssem.at[m], p_rsem.at[m], at_ep(1))
    answers = {}
    for m in far:
        paired[m].wait_recv()
        zsend[m // 2] = (yhold[flip(me, m)] + ypair[m // 2].astype(F32)).astype(BF16)
        answers[m] = send(zsend.at[m // 2], zrecv.at[m // 2], y_ssem.at[m], y_rsem.at[m], at_ep(m))
    paired[0].wait_recv()
    combined = yown[...] + yhold[me] + ypair[0].astype(F32)
    copies["outg"].wait()
    for m in far:
        answers[m].wait_recv()
        combined = combined + zrecv[m // 2].astype(F32)

    squared = combined * combined
    lanes = squared[:, :LANES]
    for c in range(LANES, dim, LANES):
        lanes = lanes + squared[:, c : c + LANES]
    sq_all[mine] = lanes
    last = [
        send(sq_all.at[mine], sq_all.at[mine], q_ssem.at[m], q_rsem.at[m], at_tp(m)) for m in tp_masks
    ]
    scaled = combined * flat_gain(outg_ref)
    for copy in last:
        copy.wait_recv()
    lanes = sq_all[0]
    for q in range(1, n_tp):
        lanes = lanes + sq_all[q]
    mean = jnp.sum(lanes, axis=1, keepdims=True) / width
    o_ref[...] = (scaled * lax.rsqrt(mean + 1e-06)).astype(BF16)
    for copy in pending:
        copy.wait_send()


def fused(n_ep, n_tp, tokens, routes, gates, pre_gain, eg, eu, ed, sg, su, sd, out_gain):
    tok, dim = tokens.shape
    local, _, hidden = eg.shape
    top = routes.shape[1]
    cap = max(2, 3 * tok * top // (2 * local * n_ep))
    per = n_ep * cap
    rows = local * per
    part = hidden // n_tp
    vmem, anywhere = pl.BlockSpec(memory_space=pltpu.VMEM), pl.BlockSpec(memory_space=pl.ANY)
    sems = lambda n: pltpu.SemaphoreType.DMA((n,))
    return pl.pallas_call(
        functools.partial(fused_kernel, n_ep, n_tp, cap, dim * n_tp),
        out_shape=pltpu.VMEM((tok, dim), BF16),
        in_specs=[anywhere] * 11,
        out_specs=vmem,
        scratch_shapes=[
            pltpu.VMEM((tok, dim), BF16), pltpu.VMEM((top, tok), jnp.int32), pltpu.VMEM((top, tok), F32),
            pltpu.VMEM((dim // LANES, LANES), BF16), pltpu.VMEM((dim // LANES, LANES), BF16),
            pltpu.VMEM(eg.shape, BF16), pltpu.VMEM(eu.shape, BF16), pltpu.VMEM(ed.shape, BF16),
            pltpu.VMEM(sg.shape, BF16), pltpu.VMEM(su.shape, BF16), pltpu.VMEM(sd.shape, BF16),
            pltpu.VMEM((n_ep, tok, dim + LANES), BF16),
            pltpu.VMEM((n_tp, 8, n_ep * tok), F32),
            pltpu.VMEM((rows, dim), BF16),
            pltpu.VMEM((n_tp - 1, rows, 2 * part), BF16),
            pltpu.VMEM((n_tp - 1, rows, 2 * part), BF16),
            pltpu.VMEM((rows, 2 * part), F32),
            pltpu.VMEM((n_tp - 1, tok, 2 * part), BF16),
            pltpu.VMEM((n_tp - 1, tok, 2 * part), BF16),
            pltpu.VMEM((tok, 2 * part), F32),
            pltpu.VMEM((n_tp, rows, part), BF16),
            pltpu.VMEM((n_tp, tok, part), BF16),
            pltpu.VMEM((rows, dim), F32),
            pltpu.VMEM((tok, dim), F32),
            pltpu.VMEM((n_ep, tok, dim), BF16),
            pltpu.VMEM((n_ep, tok, dim), F32),
            pltpu.VMEM((n_ep // 2, tok, dim), BF16),
            pltpu.VMEM((n_ep // 2, tok, dim), BF16),
            pltpu.VMEM((n_ep // 2, tok, dim), BF16),
            pltpu.VMEM((n_tp, tok, LANES), F32),
            sems(8 + 3 * local),
            sems(n_ep), sems(n_ep), sems(n_ep), sems(n_ep),
            sems(n_tp), sems(n_tp), sems(n_tp * local), sems(n_tp * local), sems(n_tp), sems(n_tp),
            sems(n_tp * local), sems(n_tp * local), sems(n_tp), sems(n_tp),
            sems(n_ep), sems(n_ep), sems(n_ep), sems(n_ep), sems(n_tp), sems(n_tp),
        ],
        compiler_params=pltpu.CompilerParams(
            collective_id=0, has_side_effects=True, vmem_limit_bytes=60 * 1024 * 1024
        ),
    )(
        tokens, routes.T, gates.T, pre_gain.reshape(-1, LANES), eg, eu, ed, sg, su, sd,
        out_gain.reshape(-1, LANES),
    )


def fits(n_ep, n_tp, tokens, routes, eg):
    tok, dim = tokens.shape
    local, _, hidden = eg.shape
    experts = local * n_ep
    cap = max(2, 3 * tok * routes.shape[1] // (2 * experts))
    power = (n_ep & (n_ep - 1)) == 0 and (n_tp & (n_tp - 1)) == 0
    return (
        power
        and n_ep > 1
        and n_tp > 1
        and hidden % (LANES * n_tp) == 0
        and dim % LANES == 0
        and tok % 16 == 0
        and (n_ep * cap) % 16 == 0
        and n_ep * tok == LANES
        and 4 * experts + 3 <= LANES
        and 2 * local < 8
        and n_ep > 2
    )


def per_device(*args):
    n_ep, n_tp = lax.axis_size("ep"), lax.axis_size("tp")
    if fits(n_ep, n_tp, args[0], args[1], args[4]):
        return fused(n_ep, n_tp, *args)
    return on_device(*args)


def solution(mesh):
    in_specs = (
        P("ep", "tp"),
        P("ep", None),
        P("ep", None),
        P("tp"),
        P("ep", "tp", None),
        P("ep", "tp", None),
        P("ep", None, "tp"),
        P("tp", None),
        P("tp", None),
        P(None, "tp"),
        P("tp"),
    )
    out_specs = P("ep", "tp")
    return jax.shard_map(
        per_device, mesh=mesh, in_specs=in_specs, out_specs=out_specs, check_vma=False
    )
```

```python
import functools
import jax
import jax.numpy as jnp
from jax import lax
from jax.experimental import pallas as pl
from jax.experimental.pallas import tpu as pltpu
from jax.sharding import PartitionSpec as P

D = 4096


def normalize(values, gain, squares, width):
    scale = lax.rsqrt(squares[:, None] / width + 1e-06)
    return values * scale * gain.astype(jnp.float32)


def expert_apply(buffer, expert_gate, expert_up, expert_down, shared_gate_part, shared_up_part):
    gate_part = jnp.einsum(
        "secd,edf->secf", buffer, expert_gate, preferred_element_type=jnp.float32
    )
    up_part = jnp.einsum("secd,edf->secf", buffer, expert_up, preferred_element_type=jnp.float32)
    gate_act, up_act, shared_gate_act, shared_up_act = lax.psum(
        (gate_part, up_part, shared_gate_part, shared_up_part), "tp"
    )
    hidden = (jax.nn.silu(gate_act) * up_act).astype(jnp.bfloat16)
    shared_hidden = (jax.nn.silu(shared_gate_act) * shared_up_act).astype(jnp.bfloat16)
    results = jnp.einsum(
        "secf,efd->secd", hidden, expert_down, preferred_element_type=jnp.float32
    ).astype(jnp.bfloat16)
    return (results, shared_hidden)


def on_device(
    tokens,
    routes,
    gates,
    pre_gain,
    expert_gate,
    expert_up,
    expert_down,
    shared_gate,
    shared_up,
    shared_down,
    out_gain,
):
    own_rows = tokens.astype(jnp.float32)
    in_squares = lax.psum(jnp.sum(own_rows * own_rows, axis=1), "tp")
    normed = normalize(own_rows, pre_gain, in_squares, D).astype(jnp.bfloat16)
    shared_gate_part = jnp.dot(normed, shared_gate, preferred_element_type=jnp.float32)
    shared_up_part = jnp.dot(normed, shared_up, preferred_element_type=jnp.float32)
    tok_count = tokens.shape[0]
    top_count = routes.shape[1]
    groups = lax.axis_size("ep")
    local_experts = expert_gate.shape[0]
    experts_all = local_experts * groups
    capacity = max(2, 3 * tok_count * top_count // (2 * experts_all))
    places = jnp.arange(capacity, dtype=jnp.int32)
    zero_value = jnp.zeros((), jnp.float32)
    labels = jnp.arange(experts_all, dtype=jnp.int32)
    picked = routes[:, :, None] == labels[None, None, :]
    onehot = jnp.sum(picked.astype(jnp.int32), axis=1)
    dense_gate = jnp.sum(jnp.where(picked, gates[:, :, None], zero_value), axis=1)
    slot_index = jnp.cumsum(onehot, axis=0) - onehot
    select = (slot_index.T[:, None, :] == places[None, :, None]) & (onehot.T[:, None, :] > 0)
    outgoing = jnp.einsum(
        "ect,td->ecd", select.astype(jnp.bfloat16), normed, preferred_element_type=jnp.float32
    ).astype(jnp.bfloat16)
    outgoing = outgoing.reshape(groups, local_experts, capacity, normed.shape[1])
    received = lax.all_to_all(outgoing, "ep", split_axis=0, concat_axis=0, tiled=True)
    results, shared_hidden = expert_apply(
        received, expert_gate, expert_up, expert_down, shared_gate_part, shared_up_part
    )
    returned = lax.all_to_all(results, "ep", split_axis=0, concat_axis=0, tiled=True)
    weight = jnp.where(select, dense_gate.T[:, None, :], zero_value)
    returned_rows = returned.reshape(experts_all, capacity, normed.shape[1]).astype(jnp.float32)
    routed = jnp.einsum("ect,ecd->td", weight, returned_rows, precision=lax.Precision.HIGHEST)
    shared_out = jnp.dot(shared_hidden, shared_down, preferred_element_type=jnp.float32)
    combined = routed + shared_out
    out_squares = lax.psum(jnp.sum(combined * combined, axis=1), "tp")
    return normalize(combined, out_gain, out_squares, D).astype(jnp.bfloat16)


F32 = jnp.float32
BF16 = jnp.bfloat16
LANES = 128


def flip(index, mask):
    out, bit = index, 1
    while bit <= mask:
        if mask & bit:
            out = out + bit - 2 * bit * ((index // bit) % 2)
        bit *= 2
    return out


def iota(shape, dim):
    return lax.broadcasted_iota(jnp.int32, shape, dim)


def dot(a, b):
    return jnp.dot(a, b, preferred_element_type=F32)


def batches(n_ep):
    far = list(range(2, n_ep, 2))
    return [[0] + far[:-2], far[-2:-1], far[-1:]]


def fused_kernel(
    n_ep, n_tp, cap, width,
    tok_hbm, routes_hbm, gates_hbm, pre_hbm, eg_hbm, eu_hbm, ed_hbm, sg_hbm, su_hbm, sd_hbm, outg_hbm,
    o_ref,
    tok_ref, routes_ref, gates_ref, pre_ref, outg_ref,
    wg, wu, wd, sg, su, sd,
    xall, ss_all, bufs,
    rs_send, rs_recv, rs_own, rsh_send, rsh_recv, rsh_own,
    hid, hidsh, yown, yhold, ysend, ypair, zsend, zrecv, sq_all,
    w_sem, x_send, x_recv, ss_send, ss_recv, rs_ssem, rs_rsem, rsh_ssem, rsh_rsem,
    h_ssem, h_rsem, hs_ssem, hs_rsem, p_ssem, p_rsem, y_ssem, y_rsem, q_ssem, q_rsem,
):
    me = lax.axis_index("ep")
    mine = lax.axis_index("tp")
    tok, dim = tok_ref.shape
    local = eg_hbm.shape[0]
    experts = local * n_ep
    top = routes_hbm.shape[0]
    part = eg_hbm.shape[2] // n_tp
    tp_masks = sorted(range(1, n_tp), key=lambda m: -bin(m).count("1"))
    evens = batches(n_ep)
    count = len(evens)
    order = [m for batch in evens for m in batch + [m + 1 for m in batch]]
    place = {m: i for i, m in enumerate(order)}
    owner = {m: b for b, batch in enumerate(evens) for m in batch}
    far = [m for batch in evens for m in batch if m]
    slot = {m: i for i, m in enumerate(far)}
    pairs = [len(batch) for batch in evens]
    start = [place[batch[0]] for batch in evens]
    span = [2 * p * tok for p in pairs]
    per = [2 * p * cap for p in pairs]
    rows = [local * p for p in per]

    def at_ep(mask):
        return {"ep": flip(me, mask)}

    def at_tp(mask):
        return {"tp": flip(mine, mask)}

    barrier = pltpu.get_barrier_semaphore()
    for m in far + [1]:
        pl.semaphore_signal(barrier, inc=1, device_id=at_ep(m), device_id_type=pl.DeviceIdType.MESH)
    for m in range(1, n_tp):
        pl.semaphore_signal(barrier, inc=1, device_id=at_tp(m), device_id_type=pl.DeviceIdType.MESH)

    copies = {}
    loads = (
        ("routes", routes_hbm, routes_ref), ("gates", gates_hbm, gates_ref), ("tok", tok_hbm, tok_ref),
        ("pre", pre_hbm, pre_ref), ("sg", sg_hbm, sg), ("su", su_hbm, su), ("g", eg_hbm, wg), ("u", eu_hbm, wu),
        ("sd", sd_hbm, sd), ("d", ed_hbm, wd), ("outg", outg_hbm, outg_ref),
    )
    for i, (name, src, dst) in enumerate(loads):
        copies[name] = pltpu.make_async_copy(src, dst, w_sem.at[i])
        copies[name].start()

    def describe(src, dst, ssem, rsem, where):
        return pltpu.make_async_remote_copy(
            src_ref=src, dst_ref=dst, send_sem=ssem, recv_sem=rsem,
            device_id=where, device_id_type=pl.DeviceIdType.MESH,
        )

    def send(src, dst, ssem, rsem, where):
        describe(src, dst, ssem, rsem, where).start()

    def arrived(ref, ssem, rsem, where):
        describe(ref, ref, ssem, rsem, where).wait_recv()

    def sent(ref, ssem, rsem, where):
        describe(ref, ref, ssem, rsem, where).wait_send()

    def flat_gain(ref):
        value = ref[...].astype(F32)
        return jnp.concatenate([value[i : i + 1, :] for i in range(ref.shape[0])], axis=1)

    ss_all[:, 0] = jnp.zeros((ss_all.shape[0],) + ss_all.shape[2:], F32)
    copies["routes"].wait()
    copies["gates"].wait()
    row = iota((LANES, tok), 0)
    names = row % experts
    dense = jnp.zeros((LANES, tok), F32)
    for k in range(top):
        dense = dense + jnp.where(routes_ref[k : k + 1, :] == names, gates_ref[k : k + 1, :], 0.0)
    earlier = jnp.where(iota((tok, tok), 0) < iota((tok, tok), 1), 1.0, 0.0).astype(BF16)
    slots = dot(jnp.where(dense > 0.0, 1.0, 0.0).astype(BF16), earlier)
    slots = jnp.where(dense > 0.0, slots + 1.0, 0.0)

    def terms(value):
        hi = value.astype(BF16).astype(F32)
        mid = (value - hi).astype(BF16).astype(F32)
        return hi, mid, value - hi - mid

    def choose(index, values):
        out = 0.0
        for i, value in enumerate(values):
            out = jnp.where(index == i, value, out)
        return out

    listed = choose(row // experts, terms(dense) + (slots,)).astype(BF16)
    eye = jnp.where(iota((tok, tok), 0) == iota((tok, tok), 1), 1.0, 0.0).astype(BF16)
    meta = lax.dot_general(eye, listed, (((1,), (1,)), ((), ())), preferred_element_type=F32)
    copies["tok"].wait()
    copies["pre"].wait()
    x = tok_ref[...].astype(F32)
    xall[0, :, :dim] = (x * flat_gain(pre_ref)).astype(BF16)
    squares = jnp.sum(x * x, axis=1, keepdims=True)
    lane = iota((tok, LANES), 1)
    meta = jnp.where(lane < 4 * experts, meta, choose(lane - 4 * experts, terms(squares)))
    xall[0, :, dim:] = meta.astype(BF16)

    pl.semaphore_wait(barrier, len(far) + 1 + n_tp - 1)

    def x_to(m, held, put, index):
        send(xall.at[held], xall.at[put], x_send.at[0], x_recv.at[index], at_ep(m))

    odd = len(far)
    x_to(1, 0, place[1], odd)
    for m in far:
        x_to(m, 0, place[m], slot[m])

    def relay(m):
        arrived(xall.at[place[m]], x_send.at[0], x_recv.at[slot[m]], at_ep(m))
        x_to(1, place[m], place[m + 1], odd + owner[m])

    def columns(m):
        return pl.ds(pl.multiple_of(flip(mine, m) * part, part), part)

    xs = xall[0, :, :dim]
    def shared_pieces():
      copies["sg"].wait()
      copies["su"].wait()
      for m in tp_masks + [0]:
        g = dot(xs, sg[:, columns(m)])
        u = dot(xs, su[:, columns(m)])
        if m:
            rsh_send[m - 1, :, :part] = g.astype(BF16)
            rsh_send[m - 1, :, part:] = u.astype(BF16)
            send(rsh_send.at[m - 1], rsh_recv.at[m - 1], rsh_ssem.at[0], rsh_rsem.at[0], at_tp(m))
        else:
            rsh_own[:, :part] = g
            rsh_own[:, part:] = u

    shared_pieces()

    def odds(b):
        return xall.at[pl.ds(start[b] + pairs[b], pairs[b])]

    row8, lane8 = iota((8, LANES), 0), iota((8, LANES), 1)
    gate_lane = lane8 < 3 * experts
    slot_lane = (lane8 >= 3 * experts) & (lane8 < 4 * experts)
    mine8 = me * local + row8
    pick = (
        ((row8 < local) & gate_lane & (lane8 % experts == mine8))
        | ((row8 == local) & (lane8 >= 4 * experts))
        | ((row8 > local) & (row8 <= 2 * local) & slot_lane & (lane8 % experts == mine8 - local - 1))
    )
    pick = jnp.where(pick, 1.0, 0.0).astype(BF16)
    tables, chosen, scale, own = {}, {}, {}, {}

    def gather(b):
        arrived(odds(b), x_send.at[0], x_recv.at[odd + b], at_ep(1))
        blocks = pl.ds(start[b], 2 * pairs[b])
        tail = xall[blocks, :, dim:].reshape(span[b], LANES)
        table = lax.dot_general(pick, tail, (((1,), (1,)), ((), ())), preferred_element_type=F32)
        ss_all[b, 0, :, : span[b]] = table[local : local + 1, :]
        for m in tp_masks:
            send(ss_all.at[b, 0], ss_all.at[b, m], ss_send.at[0], ss_recv.at[b], at_tp(m))
        first = (iota((8, span[b]), 1) // tok) * cap - 1
        target = jnp.where(table > 0.5, first + table.astype(jnp.int32), -rows[b])
        pieces = [
            jnp.where(iota((rows[b], span[b]), 0) == target[local + 1 + e : local + 2 + e, :] + e * per[b], 1.0, 0.0)
            for e in range(local)
        ]
        tables[b], chosen[b] = table, pieces
        flat = xall[blocks, :, :dim].reshape(span[b], dim)
        for e in range(local):
            bufs[b][e] = dot(pieces[e].astype(BF16), flat).astype(BF16)

    def piece(b, m):
        g, u = 0.0, 0.0
        for e in range(local):
            rhs = bufs[b][e]
            g = g + dot(rhs, wg[e, :, columns(m)])
            u = u + dot(rhs, wu[e, :, columns(m)])
        if m:
            rs_send[b][m - 1, :, :part] = g.astype(BF16)
            rs_send[b][m - 1, :, part:] = u.astype(BF16)
            send(rs_send[b].at[m - 1], rs_recv[b].at[m - 1], rs_ssem.at[b], rs_rsem.at[b], at_tp(m))
        else:
            rs_own[b][:, :part] = g
            rs_own[b][:, part:] = u

    def scales(b):
        arrived(ss_all.at[b, pl.ds(1, n_tp - 1)], ss_send.at[0], ss_recv.at[b], at_tp(1))
        ss = ss_all[b, 0, :, : span[b]]
        for m in range(1, n_tp):
            ss = ss + ss_all[b, m, :, : span[b]]
        scale[b] = lax.rsqrt(ss / width + 1e-06)

    def activate(sums, by):
        g, u = sums[:, :part] * by, sums[:, part:] * by
        return (g / (1.0 + jnp.exp(-g)) * u).astype(BF16)

    def act(b):
        by = jnp.sum(sum(chosen[b]) * scale[b], axis=1, keepdims=True)
        arrived(rs_recv[b], rs_ssem.at[b], rs_rsem.at[b], at_tp(1))
        sums = rs_own[b][...]
        for m in tp_masks:
            sums = sums + rs_recv[b][m - 1].astype(F32)
        hid[b][0] = activate(sums, by)
        for m in tp_masks:
            send(hid[b].at[0], hid[b].at[m], h_ssem.at[b], h_rsem.at[b], at_tp(m))

    def down(b, m, e):
        depth = pl.ds(pl.multiple_of(flip(mine, m) * part, part), part)
        return dot(hid[b][m], wd[e, depth, :])

    def down_own(b):
        own[b] = [down(b, 0, e) for e in range(local)]

    def ypart(b):
        return pl.ds(start[b] // 2, pairs[b])

    def back(b):
        arrived(hid[b].at[pl.ds(1, n_tp - 1)], h_ssem.at[b], h_rsem.at[b], at_tp(1))
        gated = 0.0
        for e in range(local):
            acc = own[b][e]
            for m in tp_masks[::-1]:
                acc = acc + down(b, m, e)
            gated = gated + acc * jnp.sum(chosen[b][e] * tables[b][e : e + 1, :], axis=1, keepdims=True)
        y = lax.dot_general(
            sum(chosen[b]).astype(BF16), gated.astype(BF16), (((0,), (0,)), ((), ())), preferred_element_type=F32
        ).reshape(2 * pairs[b], tok, dim)
        ysend[ypart(b)] = y[pairs[b] :].astype(BF16)
        yhold[ypart(b)] = y[: pairs[b]]
        send(ysend.at[ypart(b)], ypair.at[ypart(b)], p_ssem.at[0], p_rsem.at[b], at_ep(1))

    def forward(b):
        arrived(ypair.at[ypart(b)], p_ssem.at[0], p_rsem.at[b], at_ep(1))
        for i, m in enumerate(evens[b]):
            both = yhold[start[b] // 2 + i] + ypair[start[b] // 2 + i].astype(F32)
            if m:
                zsend[slot[m]] = both.astype(BF16)
                send(zsend.at[slot[m]], zrecv.at[slot[m]], y_ssem.at[0], y_rsem.at[b], at_ep(m))
            else:
                kept.append(both)

    def shared_act():
        match = jnp.where(iota((tok, span[0]), 1) == iota((tok, span[0]), 0), 1.0, 0.0)
        by = jnp.sum(match * scale[0], axis=1, keepdims=True)
        arrived(rsh_recv, rsh_ssem.at[0], rsh_rsem.at[0], at_tp(1))
        sums = rsh_own[...]
        for m in tp_masks:
            sums = sums + rsh_recv[m - 1].astype(F32)
        hidsh[0] = activate(sums, by)
        for m in tp_masks:
            send(hidsh.at[0], hidsh.at[m], hs_ssem.at[0], hs_rsem.at[0], at_tp(m))

    def shared_down():
        arrived(hidsh.at[pl.ds(1, n_tp - 1)], hs_ssem.at[0], hs_rsem.at[0], at_tp(1))
        shared_out = 0.0
        for m in range(n_tp):
            depth = pl.ds(pl.multiple_of(flip(mine, m) * part, part), part)
            shared_out = shared_out + dot(hidsh[m], sd[depth, :])
        yown[...] = shared_out

    kept = []
    for m in evens[0][1:]:
        relay(m)
    gather(0)
    copies["g"].wait()
    copies["u"].wait()
    piece(0, tp_masks[0])
    for m in evens[1]:
        relay(m)
    for m in tp_masks[1:] + [0]:
        piece(0, m)
    gather(1)
    for m in evens[2]:
        relay(m)
    for m in tp_masks:
        piece(1, m)
    gather(2)
    for m in tp_masks:
        piece(2, m)
    scales(0)
    act(0)
    shared_act()
    piece(1, 0)
    scales(1)
    act(1)
    piece(2, 0)
    copies["d"].wait()
    copies["sd"].wait()
    down_own(0)
    down_own(1)
    scales(2)
    act(2)
    back(0)
    shared_down()
    back(1)
    forward(0)
    down_own(2)
    back(2)
    forward(1)
    forward(2)
    combined = yown[...]
    for both in kept:
        combined = combined + both
    copies["outg"].wait()
    for b, batch in enumerate(evens):
        held = [slot[m] for m in batch if m]
        if held:
            arrived(zrecv.at[pl.ds(held[0], len(held))], y_ssem.at[0], y_rsem.at[b], at_ep(2))
            for i in held:
                combined = combined + zrecv[i].astype(F32)

    squared = combined * combined
    lanes = squared[:, :LANES]
    for c in range(LANES, dim, LANES):
        lanes = lanes + squared[:, c : c + LANES]
    sq_all[0] = lanes
    for m in tp_masks:
        send(sq_all.at[0], sq_all.at[m], q_ssem.at[0], q_rsem.at[0], at_tp(m))
    scaled = combined * flat_gain(outg_ref)
    arrived(sq_all.at[pl.ds(1, n_tp - 1)], q_ssem.at[0], q_rsem.at[0], at_tp(1))
    lanes = sq_all[0]
    for m in range(1, n_tp):
        lanes = lanes + sq_all[m]
    mean = jnp.sum(lanes, axis=1, keepdims=True) / width
    o_ref[...] = (scaled * lax.rsqrt(mean + 1e-06)).astype(BF16)
    sent(xall.at[pl.ds(0, n_ep - 1)], x_send.at[0], x_recv.at[0], at_ep(1))
    sent(ss_all.at[:, pl.ds(1, n_tp - 1)], ss_send.at[0], ss_recv.at[0], at_tp(1))
    sent(rsh_send, rsh_ssem.at[0], rsh_rsem.at[0], at_tp(1))
    for b in range(count):
        sent(rs_send[b], rs_ssem.at[b], rs_rsem.at[b], at_tp(1))
        sent(hid[b].at[pl.ds(1, n_tp - 1)], h_ssem.at[b], h_rsem.at[b], at_tp(1))
    sent(hidsh.at[pl.ds(1, n_tp - 1)], hs_ssem.at[0], hs_rsem.at[0], at_tp(1))
    sent(ysend, p_ssem.at[0], p_rsem.at[0], at_ep(1))
    sent(zsend, y_ssem.at[0], y_rsem.at[0], at_ep(2))
    sent(sq_all.at[pl.ds(1, n_tp - 1)], q_ssem.at[0], q_rsem.at[0], at_tp(1))


def fused(n_ep, n_tp, tokens, routes, gates, pre_gain, eg, eu, ed, sg, su, sd, out_gain):
    tok, dim = tokens.shape
    local, _, hidden = eg.shape
    top = routes.shape[1]
    cap = max(2, 3 * tok * top // (2 * local * n_ep))
    half = n_ep // 2
    evens = batches(n_ep)
    count = len(evens)
    rows = [local * 2 * len(batch) * cap for batch in evens]
    part = hidden // n_tp
    anywhere = pl.BlockSpec(memory_space=pl.ANY)
    sems = lambda n: pltpu.SemaphoreType.DMA((n,))
    return pl.pallas_call(
        functools.partial(fused_kernel, n_ep, n_tp, cap, dim * n_tp),
        out_shape=pltpu.VMEM((tok, dim), BF16),
        in_specs=[anywhere] * 11,
        out_specs=pl.BlockSpec(memory_space=pltpu.VMEM),
        scratch_shapes=[
            pltpu.VMEM((tok, dim), BF16), pltpu.VMEM((top, tok), jnp.int32), pltpu.VMEM((top, tok), F32),
            pltpu.VMEM((dim // LANES, LANES), BF16), pltpu.VMEM((dim // LANES, LANES), BF16),
            pltpu.VMEM(eg.shape, BF16), pltpu.VMEM(eu.shape, BF16), pltpu.VMEM(ed.shape, BF16),
            pltpu.VMEM(sg.shape, BF16), pltpu.VMEM(su.shape, BF16), pltpu.VMEM(sd.shape, BF16),
            pltpu.VMEM((n_ep, tok, dim + LANES), BF16),
            pltpu.VMEM((count, n_tp, 1, LANES), F32),
            [pltpu.VMEM((local, r, dim), BF16) for r in rows],
            [pltpu.VMEM((n_tp - 1, r, 2 * part), BF16) for r in rows],
            [pltpu.VMEM((n_tp - 1, r, 2 * part), BF16) for r in rows],
            [pltpu.VMEM((r, 2 * part), F32) for r in rows],
            pltpu.VMEM((n_tp - 1, tok, 2 * part), BF16),
            pltpu.VMEM((n_tp - 1, tok, 2 * part), BF16),
            pltpu.VMEM((tok, 2 * part), F32),
            [pltpu.VMEM((n_tp, r, part), BF16) for r in rows],
            pltpu.VMEM((n_tp, tok, part), BF16),
            pltpu.VMEM((tok, dim), F32),
            pltpu.VMEM((half, tok, dim), F32),
            pltpu.VMEM((half, tok, dim), BF16),
            pltpu.VMEM((half, tok, dim), BF16),
            pltpu.VMEM((half - 1, tok, dim), BF16),
            pltpu.VMEM((half - 1, tok, dim), BF16),
            pltpu.VMEM((n_tp, tok, LANES), F32),
            sems(11),
            sems(1), sems(half - 1 + count), sems(1), sems(count), sems(count), sems(count), sems(1), sems(1),
            sems(count), sems(count), sems(1), sems(1), sems(1), sems(count), sems(1), sems(count), sems(1), sems(1),
        ],
        compiler_params=pltpu.CompilerParams(
            collective_id=0, has_side_effects=True, vmem_limit_bytes=60 * 1024 * 1024
        ),
    )(
        tokens, routes.T, gates.T, pre_gain.reshape(-1, LANES), eg, eu, ed, sg, su, sd,
        out_gain.reshape(-1, LANES),
    )


def fits(n_ep, n_tp, tokens, routes, eg):
    tok, dim = tokens.shape
    local, _, hidden = eg.shape
    experts = local * n_ep
    cap = max(2, 3 * tok * routes.shape[1] // (2 * experts))
    power = (n_ep & (n_ep - 1)) == 0 and (n_tp & (n_tp - 1)) == 0
    return (
        power
        and n_ep > 4
        and n_tp > 1
        and hidden % (LANES * n_tp) == 0
        and dim % LANES == 0
        and tok % 16 == 0
        and n_ep * tok == LANES
        and 4 * experts + 3 <= LANES
        and 2 * local < 8
    )


def per_device(*args):
    n_ep, n_tp = lax.axis_size("ep"), lax.axis_size("tp")
    if fits(n_ep, n_tp, args[0], args[1], args[4]):
        return fused(n_ep, n_tp, *args)
    return on_device(*args)


def solution(mesh):
    in_specs = (
        P("ep", "tp"),
        P("ep", None),
        P("ep", None),
        P("tp"),
        P("ep", "tp", None),
        P("ep", "tp", None),
        P("ep", None, "tp"),
        P("tp", None),
        P("tp", None),
        P(None, "tp"),
        P("tp"),
    )
    out_specs = P("ep", "tp")
    return jax.shard_map(
        per_device, mesh=mesh, in_specs=in_specs, out_specs=out_specs, check_vma=False
    )
```

```python
import functools
import jax
import jax.numpy as jnp
from jax import lax
from jax.experimental import pallas as pl
from jax.experimental.pallas import tpu as pltpu
from jax.sharding import PartitionSpec as P

D = 4096


def normalize(values, gain, squares, width):
    scale = lax.rsqrt(squares[:, None] / width + 1e-06)
    return values * scale * gain.astype(jnp.float32)


def expert_apply(buffer, expert_gate, expert_up, expert_down, shared_gate_part, shared_up_part):
    gate_part = jnp.einsum(
        "secd,edf->secf", buffer, expert_gate, preferred_element_type=jnp.float32
    )
    up_part = jnp.einsum("secd,edf->secf", buffer, expert_up, preferred_element_type=jnp.float32)
    gate_act, up_act, shared_gate_act, shared_up_act = lax.psum(
        (gate_part, up_part, shared_gate_part, shared_up_part), "tp"
    )
    hidden = (jax.nn.silu(gate_act) * up_act).astype(jnp.bfloat16)
    shared_hidden = (jax.nn.silu(shared_gate_act) * shared_up_act).astype(jnp.bfloat16)
    results = jnp.einsum(
        "secf,efd->secd", hidden, expert_down, preferred_element_type=jnp.float32
    ).astype(jnp.bfloat16)
    return (results, shared_hidden)


def on_device(
    tokens,
    routes,
    gates,
    pre_gain,
    expert_gate,
    expert_up,
    expert_down,
    shared_gate,
    shared_up,
    shared_down,
    out_gain,
):
    own_rows = tokens.astype(jnp.float32)
    in_squares = lax.psum(jnp.sum(own_rows * own_rows, axis=1), "tp")
    normed = normalize(own_rows, pre_gain, in_squares, D).astype(jnp.bfloat16)
    shared_gate_part = jnp.dot(normed, shared_gate, preferred_element_type=jnp.float32)
    shared_up_part = jnp.dot(normed, shared_up, preferred_element_type=jnp.float32)
    tok_count = tokens.shape[0]
    top_count = routes.shape[1]
    groups = lax.axis_size("ep")
    local_experts = expert_gate.shape[0]
    experts_all = local_experts * groups
    capacity = max(2, 3 * tok_count * top_count // (2 * experts_all))
    places = jnp.arange(capacity, dtype=jnp.int32)
    zero_value = jnp.zeros((), jnp.float32)
    labels = jnp.arange(experts_all, dtype=jnp.int32)
    picked = routes[:, :, None] == labels[None, None, :]
    onehot = jnp.sum(picked.astype(jnp.int32), axis=1)
    dense_gate = jnp.sum(jnp.where(picked, gates[:, :, None], zero_value), axis=1)
    slot_index = jnp.cumsum(onehot, axis=0) - onehot
    select = (slot_index.T[:, None, :] == places[None, :, None]) & (onehot.T[:, None, :] > 0)
    outgoing = jnp.einsum(
        "ect,td->ecd", select.astype(jnp.bfloat16), normed, preferred_element_type=jnp.float32
    ).astype(jnp.bfloat16)
    outgoing = outgoing.reshape(groups, local_experts, capacity, normed.shape[1])
    received = lax.all_to_all(outgoing, "ep", split_axis=0, concat_axis=0, tiled=True)
    results, shared_hidden = expert_apply(
        received, expert_gate, expert_up, expert_down, shared_gate_part, shared_up_part
    )
    returned = lax.all_to_all(results, "ep", split_axis=0, concat_axis=0, tiled=True)
    weight = jnp.where(select, dense_gate.T[:, None, :], zero_value)
    returned_rows = returned.reshape(experts_all, capacity, normed.shape[1]).astype(jnp.float32)
    routed = jnp.einsum("ect,ecd->td", weight, returned_rows, precision=lax.Precision.HIGHEST)
    shared_out = jnp.dot(shared_hidden, shared_down, preferred_element_type=jnp.float32)
    combined = routed + shared_out
    out_squares = lax.psum(jnp.sum(combined * combined, axis=1), "tp")
    return normalize(combined, out_gain, out_squares, D).astype(jnp.bfloat16)


F32 = jnp.float32
BF16 = jnp.bfloat16
LANES = 128


def flip(index, mask):
    out, bit = index, 1
    while bit <= mask:
        if mask & bit:
            out = out + bit - 2 * bit * ((index // bit) % 2)
        bit *= 2
    return out


def iota(shape, dim):
    return lax.broadcasted_iota(jnp.int32, shape, dim)


def dot(a, b):
    return jnp.dot(a, b, preferred_element_type=F32)


def batches(n_ep):
    far = list(range(2, n_ep, 2))
    return [[0], far[-2::-1], far[-1:]]


def fused_kernel(
    n_ep, n_tp, cap, width,
    tok_hbm, routes_hbm, gates_hbm, pre_hbm, eg_hbm, eu_hbm, ed_hbm, sg_hbm, su_hbm, sd_hbm, outg_hbm,
    o_ref,
    tok_ref, routes_ref, gates_ref, pre_ref, outg_ref,
    wg, wu, wd, sg, su, sd,
    xall, ss_all, bufs,
    rs_send, rs_recv, rsh_send, rsh_recv, rsh_own,
    hid_out, hid, hidsh, yown, yhold, ysend, ypair, zsend, zrecv, sq_all,
    w_sem, x_send, x_recv, ss_send, ss_recv, rs_ssem, rs_rsem, rsh_ssem, rsh_rsem,
    h_ssem, h_rsem, hs_ssem, hs_rsem, p_ssem, p_rsem, y_ssem, y_rsem, q_ssem, q_rsem,
):
    me = lax.axis_index("ep")
    mine = lax.axis_index("tp")
    tok, dim = tok_ref.shape
    local = eg_hbm.shape[0]
    experts = local * n_ep
    top = routes_hbm.shape[0]
    part = eg_hbm.shape[2] // n_tp
    tp_masks = sorted(range(1, n_tp), key=lambda m: -bin(m).count("1"))
    evens = batches(n_ep)
    count = len(evens)
    order = [m for batch in evens for m in batch + [m + 1 for m in batch]]
    place = {m: i for i, m in enumerate(order)}
    owner = {m: b for b, batch in enumerate(evens) for m in batch}
    far = [m for batch in evens for m in batch if m]
    slot = {m: i for i, m in enumerate(far)}
    pairs = [len(batch) for batch in evens]
    start = [place[batch[0]] for batch in evens]
    span = [2 * p * tok for p in pairs]
    per = [2 * p * cap for p in pairs]
    rows = [local * p for p in per]

    def at_ep(mask):
        return {"ep": flip(me, mask)}

    def at_tp(mask):
        return {"tp": flip(mine, mask)}

    def across(mask):
        return {"ep": flip(me, 1), "tp": flip(mine, mask)}

    barrier = pltpu.get_barrier_semaphore()
    peers = [at_ep(m + 1) for m in [0] + far]
    peers += [where(m) for m in range(1, n_tp) for where in (at_tp, across)]
    for where in peers:
        pl.semaphore_signal(barrier, inc=1, device_id=where, device_id_type=pl.DeviceIdType.MESH)

    def columns(m):
        return pl.ds(pl.multiple_of(flip(mine, m) * part, part), part)

    copies = {}
    loads = (
        ("routes", routes_hbm, routes_ref), ("gates", gates_hbm, gates_ref), ("tok", tok_hbm, tok_ref),
        ("pre", pre_hbm, pre_ref),
    )
    for m in tp_masks + [0]:
        here = (slice(None), slice(None), columns(m))
        loads += ((("g", m), eg_hbm.at[here], wg.at[here]), (("u", m), eu_hbm.at[here], wu.at[here]))
    loads += (
        ("sg", sg_hbm, sg), ("su", su_hbm, su), ("sd", sd_hbm, sd), ("d", ed_hbm, wd), ("outg", outg_hbm, outg_ref),
    )
    for i, (name, src, dst) in enumerate(loads):
        copies[name] = pltpu.make_async_copy(src, dst, w_sem.at[i])
        if name not in ("sd", "d", "outg"):
            copies[name].start()

    def describe(src, dst, ssem, rsem, where):
        return pltpu.make_async_remote_copy(
            src_ref=src, dst_ref=dst, send_sem=ssem, recv_sem=rsem,
            device_id=where, device_id_type=pl.DeviceIdType.MESH,
        )

    def send(src, dst, ssem, rsem, where):
        describe(src, dst, ssem, rsem, where).start()

    def arrived(ref, ssem, rsem, where):
        describe(ref, ref, ssem, rsem, where).wait_recv()

    def sent(ref, ssem, rsem, where):
        describe(ref, ref, ssem, rsem, where).wait_send()

    def flat_gain(ref):
        value = ref[...].astype(F32)
        return jnp.concatenate([value[i : i + 1, :] for i in range(ref.shape[0])], axis=1)

    ss_all[:, 0] = jnp.zeros((ss_all.shape[0],) + ss_all.shape[2:], F32)
    copies["routes"].wait()
    copies["gates"].wait()
    row = iota((LANES, tok), 0)
    names = row % experts
    dense = jnp.zeros((LANES, tok), F32)
    for k in range(top):
        dense = dense + jnp.where(routes_ref[k : k + 1, :] == names, gates_ref[k : k + 1, :], 0.0)
    earlier = jnp.where(iota((tok, tok), 0) < iota((tok, tok), 1), 1.0, 0.0).astype(BF16)
    slots = dot(jnp.where(dense > 0.0, 1.0, 0.0).astype(BF16), earlier)
    slots = jnp.where(dense > 0.0, slots + 1.0, 0.0)

    def terms(value):
        hi = value.astype(BF16).astype(F32)
        mid = (value - hi).astype(BF16).astype(F32)
        return hi, mid, value - hi - mid

    def choose(index, values):
        out = 0.0
        for i, value in enumerate(values):
            out = jnp.where(index == i, value, out)
        return out

    listed = choose(row // experts, terms(dense) + (slots,)).astype(BF16)
    eye = jnp.where(iota((tok, tok), 0) == iota((tok, tok), 1), 1.0, 0.0).astype(BF16)
    meta = lax.dot_general(eye, listed, (((1,), (1,)), ((), ())), preferred_element_type=F32)
    copies["tok"].wait()
    copies["pre"].wait()
    x = tok_ref[...].astype(F32)
    xall[0, :, :dim] = (x * flat_gain(pre_ref)).astype(BF16)
    squares = jnp.sum(x * x, axis=1, keepdims=True)
    lane = iota((tok, LANES), 1)
    meta = jnp.where(lane < 4 * experts, meta, choose(lane - 4 * experts, terms(squares)))
    xall[0, :, dim:] = meta.astype(BF16)

    pl.semaphore_wait(barrier, len(peers))

    def x_to(m, held, put, index):
        send(xall.at[held], xall.at[put], x_send.at[0], x_recv.at[index], at_ep(m))

    odd = len(far)
    x_to(1, 0, place[1], odd)
    for m in far[-2::-1] + far[-1:]:
        x_to(m + 1, 0, place[m + 1], slot[m])

    def relay(m):
        arrived(xall.at[place[m + 1]], x_send.at[0], x_recv.at[slot[m]], at_ep(m + 1))
        x_to(1, place[m + 1], place[m], odd + owner[m])

    xs = xall[0, :, :dim]
    def shared_piece(m):
        g = dot(xs, sg[:, columns(m)])
        u = dot(xs, su[:, columns(m)])
        if m:
            rsh_send[m - 1, :, :part] = g.astype(BF16)
            rsh_send[m - 1, :, part:] = u.astype(BF16)
            send(rsh_send.at[m - 1], rsh_recv.at[m - 1], rsh_ssem.at[0], rsh_rsem.at[0], at_tp(m))
        else:
            rsh_own[:, :part] = g
            rsh_own[:, part:] = u

    def from_pair(b):
        return xall.at[pl.ds(start[b] if b else place[1], pairs[b])]

    row8, lane8 = iota((8, LANES), 0), iota((8, LANES), 1)
    gate_lane = lane8 < 3 * experts
    slot_lane = (lane8 >= 3 * experts) & (lane8 < 4 * experts)
    mine8 = me * local + row8
    pair8 = flip(me, 1) * local + row8
    pick = (
        ((row8 < local) & gate_lane & (lane8 % experts == mine8))
        | ((row8 == local) & (lane8 >= 4 * experts))
        | ((row8 > local) & (row8 <= 2 * local) & slot_lane & (lane8 % experts == mine8 - local - 1))
        | ((row8 > 2 * local) & (row8 <= 3 * local) & slot_lane & (lane8 % experts == pair8 - 2 * local - 1))
    )
    pick = jnp.where(pick, 1.0, 0.0).astype(BF16)
    tables, chosen, others, scale, own = {}, {}, {}, {}, {}

    def gather(b):
        arrived(from_pair(b), x_send.at[0], x_recv.at[odd + b], at_ep(1))
        blocks = pl.ds(start[b], 2 * pairs[b])
        tail = xall[blocks, :, dim:].reshape(span[b], LANES)
        table = lax.dot_general(pick, tail, (((1,), (1,)), ((), ())), preferred_element_type=F32)
        ss_all[b, 0, :, : span[b]] = table[local : local + 1, :]
        for m in tp_masks:
            send(ss_all.at[b, 0], ss_all.at[b, m], ss_send.at[0], ss_recv.at[b], at_tp(m))
        block = iota((8, span[b]), 1) // tok
        seen = (block + pairs[b]) % (2 * pairs[b])
        block = jnp.where(iota((8, span[b]), 0) > 2 * local, seen, block)
        target = jnp.where(table > 0.5, block * cap - 1 + table.astype(jnp.int32), -rows[b])

        def piece_of(e, base):
            goal = target[base + e : base + e + 1, :] + e * per[b]
            return jnp.where(iota((rows[b], span[b]), 0) == goal, 1.0, 0.0)

        pieces = [piece_of(e, local + 1) for e in range(local)]
        others[b] = sum(piece_of(e, 2 * local + 1) for e in range(local))
        tables[b], chosen[b] = table, pieces
        flat = xall[blocks, :, :dim].reshape(span[b], dim)
        for e in range(local):
            bufs[b][e] = dot(pieces[e].astype(BF16), flat).astype(BF16)

    def piece(b, m):
        if b == 0:
            copies["g", m].wait()
            copies["u", m].wait()
        g, u = 0.0, 0.0
        for e in range(local):
            rhs = bufs[b][e]
            g = g + dot(rhs, wg[e, :, columns(m)])
            u = u + dot(rhs, wu[e, :, columns(m)])
        rs_send[b][m, :, :part] = g.astype(BF16)
        rs_send[b][m, :, part:] = u.astype(BF16)
        send(rs_send[b].at[m], rs_recv[b].at[m], rs_ssem.at[b], rs_rsem.at[b], across(m))

    def scales(b):
        arrived(ss_all.at[b, pl.ds(1, n_tp - 1)], ss_send.at[0], ss_recv.at[b], at_tp(1))
        ss = ss_all[b, 0, :, : span[b]]
        for m in range(1, n_tp):
            ss = ss + ss_all[b, m, :, : span[b]]
        scale[b] = lax.rsqrt(ss / width + 1e-06)

    def activate(sums, by):
        g, u = sums[:, :part] * by, sums[:, part:] * by
        return (g / (1.0 + jnp.exp(-g)) * u).astype(BF16)

    def act(b):
        by = jnp.sum(others[b] * scale[b], axis=1, keepdims=True)
        arrived(rs_recv[b], rs_ssem.at[b], rs_rsem.at[b], across(1))
        sums = rs_recv[b][0].astype(F32)
        for m in tp_masks:
            sums = sums + rs_recv[b][m].astype(F32)
        hid_out[b][...] = activate(sums, by)
        for m in tp_masks:
            send(hid_out[b], hid[b].at[m], h_ssem.at[b], h_rsem.at[b], across(m))
        send(hid_out[b], hid[b].at[0], h_ssem.at[b], h_rsem.at[count + b], at_ep(1))

    def down(b, m, e):
        depth = pl.ds(pl.multiple_of(flip(mine, m) * part, part), part)
        return dot(hid[b][m], wd[e, depth, :])

    def down_own(b):
        arrived(hid[b].at[0], h_ssem.at[b], h_rsem.at[count + b], at_ep(1))
        own[b] = [down(b, 0, e) for e in range(local)]

    def ypart(b):
        return pl.ds(start[b] // 2, pairs[b])

    def back(b):
        arrived(hid[b].at[pl.ds(1, n_tp - 1)], h_ssem.at[b], h_rsem.at[b], across(1))
        gated = 0.0
        for e in range(local):
            acc = own[b][e]
            for m in tp_masks[::-1]:
                acc = acc + down(b, m, e)
            gated = gated + acc * jnp.sum(chosen[b][e] * tables[b][e : e + 1, :], axis=1, keepdims=True)
        y = lax.dot_general(
            sum(chosen[b]).astype(BF16), gated.astype(BF16), (((0,), (0,)), ((), ())), preferred_element_type=F32
        ).reshape(2 * pairs[b], tok, dim)
        even, uneven = y[: pairs[b]], y[pairs[b] :]
        ysend[ypart(b)] = (even if b else uneven).astype(BF16)
        yhold[ypart(b)] = uneven if b else even
        send(ysend.at[ypart(b)], ypair.at[ypart(b)], p_ssem.at[0], p_rsem.at[b], at_ep(1))

    def forward(b):
        arrived(ypair.at[ypart(b)], p_ssem.at[0], p_rsem.at[b], at_ep(1))
        for i, m in enumerate(evens[b]):
            both = yhold[start[b] // 2 + i] + ypair[start[b] // 2 + i].astype(F32)
            if m:
                zsend[slot[m]] = both.astype(BF16)
                send(zsend.at[slot[m]], zrecv.at[slot[m]], y_ssem.at[0], y_rsem.at[b], at_ep(m + 1))
            else:
                kept.append(both)

    def shared_act():
        match = jnp.where(iota((tok, span[0]), 1) == iota((tok, span[0]), 0), 1.0, 0.0)
        by = jnp.sum(match * scale[0], axis=1, keepdims=True)
        arrived(rsh_recv, rsh_ssem.at[0], rsh_rsem.at[0], at_tp(1))
        sums = rsh_own[...]
        for m in tp_masks:
            sums = sums + rsh_recv[m - 1].astype(F32)
        hidsh[0] = activate(sums, by)
        for m in tp_masks:
            send(hidsh.at[0], hidsh.at[m], hs_ssem.at[0], hs_rsem.at[0], at_tp(m))

    def shared_down():
        arrived(hidsh.at[pl.ds(1, n_tp - 1)], hs_ssem.at[0], hs_rsem.at[0], at_tp(1))
        shared_out = 0.0
        for m in range(n_tp):
            depth = pl.ds(pl.multiple_of(flip(mine, m) * part, part), part)
            shared_out = shared_out + dot(hidsh[m], sd[depth, :])
        yown[...] = shared_out

    kept = []
    gather(0)
    for name in ("sd", "d", "outg"):
        copies[name].start()
    for m in tp_masks + [0]:
        piece(0, m)
    for m in evens[1]:
        relay(m)
    copies["sg"].wait()
    copies["su"].wait()
    for m in tp_masks + [0]:
        shared_piece(m)
    gather(1)
    piece(1, tp_masks[0])
    for m in evens[2]:
        relay(m)
    for m in tp_masks[1:]:
        piece(1, m)
    scales(0)
    act(0)
    gather(2)
    for m in tp_masks:
        piece(2, m)
    piece(1, 0)
    piece(2, 0)
    shared_act()
    copies["d"].wait()
    copies["sd"].wait()
    scales(1)
    act(1)
    scales(2)
    act(2)
    down_own(0)
    back(0)
    shared_down()
    down_own(1)
    down_own(2)
    back(1)
    back(2)
    forward(0)
    forward(1)
    forward(2)
    combined = yown[...]
    for both in kept:
        combined = combined + both
    copies["outg"].wait()
    for b, batch in enumerate(evens):
        held = [slot[m] for m in batch if m]
        if held:
            arrived(zrecv.at[pl.ds(held[0], len(held))], y_ssem.at[0], y_rsem.at[b], at_ep(3))
            for i in held:
                combined = combined + zrecv[i].astype(F32)

    squared = combined * combined
    lanes = squared[:, :LANES]
    for c in range(LANES, dim, LANES):
        lanes = lanes + squared[:, c : c + LANES]
    sq_all[0] = lanes
    for m in tp_masks:
        send(sq_all.at[0], sq_all.at[m], q_ssem.at[0], q_rsem.at[0], at_tp(m))
    scaled = combined * flat_gain(outg_ref)
    arrived(sq_all.at[pl.ds(1, n_tp - 1)], q_ssem.at[0], q_rsem.at[0], at_tp(1))
    lanes = sq_all[0]
    for m in range(1, n_tp):
        lanes = lanes + sq_all[m]
    mean = jnp.sum(lanes, axis=1, keepdims=True) / width
    o_ref[...] = (scaled * lax.rsqrt(mean + 1e-06)).astype(BF16)
    sent(xall.at[pl.ds(0, n_ep - 1)], x_send.at[0], x_recv.at[0], at_ep(1))
    sent(ss_all.at[:, pl.ds(1, n_tp - 1)], ss_send.at[0], ss_recv.at[0], at_tp(1))
    sent(rsh_send, rsh_ssem.at[0], rsh_rsem.at[0], at_tp(1))
    for b in range(count):
        sent(rs_send[b], rs_ssem.at[b], rs_rsem.at[b], across(1))
        sent(hid[b], h_ssem.at[b], h_rsem.at[b], across(1))
    sent(hidsh.at[pl.ds(1, n_tp - 1)], hs_ssem.at[0], hs_rsem.at[0], at_tp(1))
    sent(ysend, p_ssem.at[0], p_rsem.at[0], at_ep(1))
    sent(zsend, y_ssem.at[0], y_rsem.at[0], at_ep(3))
    sent(sq_all.at[pl.ds(1, n_tp - 1)], q_ssem.at[0], q_rsem.at[0], at_tp(1))


def fused(n_ep, n_tp, tokens, routes, gates, pre_gain, eg, eu, ed, sg, su, sd, out_gain):
    tok, dim = tokens.shape
    local, _, hidden = eg.shape
    top = routes.shape[1]
    cap = max(2, 3 * tok * top // (2 * local * n_ep))
    half = n_ep // 2
    evens = batches(n_ep)
    count = len(evens)
    rows = [local * 2 * len(batch) * cap for batch in evens]
    part = hidden // n_tp
    anywhere = pl.BlockSpec(memory_space=pl.ANY)
    sems = lambda n: pltpu.SemaphoreType.DMA((n,))
    return pl.pallas_call(
        functools.partial(fused_kernel, n_ep, n_tp, cap, dim * n_tp),
        out_shape=pltpu.VMEM((tok, dim), BF16),
        in_specs=[anywhere] * 11,
        out_specs=pl.BlockSpec(memory_space=pltpu.VMEM),
        scratch_shapes=[
            pltpu.VMEM((tok, dim), BF16), pltpu.VMEM((top, tok), jnp.int32), pltpu.VMEM((top, tok), F32),
            pltpu.VMEM((dim // LANES, LANES), BF16), pltpu.VMEM((dim // LANES, LANES), BF16),
            pltpu.VMEM(eg.shape, BF16), pltpu.VMEM(eu.shape, BF16), pltpu.VMEM(ed.shape, BF16),
            pltpu.VMEM(sg.shape, BF16), pltpu.VMEM(su.shape, BF16), pltpu.VMEM(sd.shape, BF16),
            pltpu.VMEM((n_ep, tok, dim + LANES), BF16),
            pltpu.VMEM((count, n_tp, 1, LANES), F32),
            [pltpu.VMEM((local, r, dim), BF16) for r in rows],
            [pltpu.VMEM((n_tp, r, 2 * part), BF16) for r in rows],
            [pltpu.VMEM((n_tp, r, 2 * part), BF16) for r in rows],
            pltpu.VMEM((n_tp - 1, tok, 2 * part), BF16),
            pltpu.VMEM((n_tp - 1, tok, 2 * part), BF16),
            pltpu.VMEM((tok, 2 * part), F32),
            [pltpu.VMEM((r, part), BF16) for r in rows],
            [pltpu.VMEM((n_tp, r, part), BF16) for r in rows],
            pltpu.VMEM((n_tp, tok, part), BF16),
            pltpu.VMEM((tok, dim), F32),
            pltpu.VMEM((half, tok, dim), F32),
            pltpu.VMEM((half, tok, dim), BF16),
            pltpu.VMEM((half, tok, dim), BF16),
            pltpu.VMEM((half - 1, tok, dim), BF16),
            pltpu.VMEM((half - 1, tok, dim), BF16),
            pltpu.VMEM((n_tp, tok, LANES), F32),
            sems(9 + 2 * n_tp),
            sems(1), sems(half - 1 + count), sems(1), sems(count), sems(count), sems(count), sems(1), sems(1),
            sems(count), sems(2 * count), sems(1), sems(1), sems(1), sems(count), sems(1), sems(count), sems(1), sems(1),
        ],
        compiler_params=pltpu.CompilerParams(
            collective_id=0, has_side_effects=True, vmem_limit_bytes=60 * 1024 * 1024
        ),
    )(
        tokens, routes.T, gates.T, pre_gain.reshape(-1, LANES), eg, eu, ed, sg, su, sd,
        out_gain.reshape(-1, LANES),
    )


def fits(n_ep, n_tp, tokens, routes, eg):
    tok, dim = tokens.shape
    local, _, hidden = eg.shape
    experts = local * n_ep
    cap = max(2, 3 * tok * routes.shape[1] // (2 * experts))
    power = (n_ep & (n_ep - 1)) == 0 and (n_tp & (n_tp - 1)) == 0
    return (
        power
        and n_ep > 4
        and n_tp > 1
        and hidden % (LANES * n_tp) == 0
        and dim % LANES == 0
        and tok % 16 == 0
        and n_ep * tok == LANES
        and 4 * experts + 3 <= LANES
        and 3 * local < 8
    )


def per_device(*args):
    n_ep, n_tp = lax.axis_size("ep"), lax.axis_size("tp")
    if fits(n_ep, n_tp, args[0], args[1], args[4]):
        return fused(n_ep, n_tp, *args)
    return on_device(*args)


def solution(mesh):
    in_specs = (
        P("ep", "tp"),
        P("ep", None),
        P("ep", None),
        P("tp"),
        P("ep", "tp", None),
        P("ep", "tp", None),
        P("ep", None, "tp"),
        P("tp", None),
        P("tp", None),
        P(None, "tp"),
        P("tp"),
    )
    out_specs = P("ep", "tp")
    return jax.shard_map(
        per_device, mesh=mesh, in_specs=in_specs, out_specs=out_specs, check_vma=False
    )
```

```python
import functools
import jax
import jax.numpy as jnp
from jax import lax
from jax.experimental import pallas as pl
from jax.experimental.pallas import tpu as pltpu
from jax.sharding import PartitionSpec as P

D = 4096


def normalize(values, gain, squares, width):
    scale = lax.rsqrt(squares[:, None] / width + 1e-06)
    return values * scale * gain.astype(jnp.float32)


def expert_apply(buffer, expert_gate, expert_up, expert_down, shared_gate_part, shared_up_part):
    gate_part = jnp.einsum(
        "secd,edf->secf", buffer, expert_gate, preferred_element_type=jnp.float32
    )
    up_part = jnp.einsum("secd,edf->secf", buffer, expert_up, preferred_element_type=jnp.float32)
    gate_act, up_act, shared_gate_act, shared_up_act = lax.psum(
        (gate_part, up_part, shared_gate_part, shared_up_part), "tp"
    )
    hidden = (jax.nn.silu(gate_act) * up_act).astype(jnp.bfloat16)
    shared_hidden = (jax.nn.silu(shared_gate_act) * shared_up_act).astype(jnp.bfloat16)
    results = jnp.einsum(
        "secf,efd->secd", hidden, expert_down, preferred_element_type=jnp.float32
    ).astype(jnp.bfloat16)
    return (results, shared_hidden)


def on_device(
    tokens,
    routes,
    gates,
    pre_gain,
    expert_gate,
    expert_up,
    expert_down,
    shared_gate,
    shared_up,
    shared_down,
    out_gain,
):
    own_rows = tokens.astype(jnp.float32)
    in_squares = lax.psum(jnp.sum(own_rows * own_rows, axis=1), "tp")
    normed = normalize(own_rows, pre_gain, in_squares, D).astype(jnp.bfloat16)
    shared_gate_part = jnp.dot(normed, shared_gate, preferred_element_type=jnp.float32)
    shared_up_part = jnp.dot(normed, shared_up, preferred_element_type=jnp.float32)
    tok_count = tokens.shape[0]
    top_count = routes.shape[1]
    groups = lax.axis_size("ep")
    local_experts = expert_gate.shape[0]
    experts_all = local_experts * groups
    capacity = max(2, 3 * tok_count * top_count // (2 * experts_all))
    places = jnp.arange(capacity, dtype=jnp.int32)
    zero_value = jnp.zeros((), jnp.float32)
    labels = jnp.arange(experts_all, dtype=jnp.int32)
    picked = routes[:, :, None] == labels[None, None, :]
    onehot = jnp.sum(picked.astype(jnp.int32), axis=1)
    dense_gate = jnp.sum(jnp.where(picked, gates[:, :, None], zero_value), axis=1)
    slot_index = jnp.cumsum(onehot, axis=0) - onehot
    select = (slot_index.T[:, None, :] == places[None, :, None]) & (onehot.T[:, None, :] > 0)
    outgoing = jnp.einsum(
        "ect,td->ecd", select.astype(jnp.bfloat16), normed, preferred_element_type=jnp.float32
    ).astype(jnp.bfloat16)
    outgoing = outgoing.reshape(groups, local_experts, capacity, normed.shape[1])
    received = lax.all_to_all(outgoing, "ep", split_axis=0, concat_axis=0, tiled=True)
    results, shared_hidden = expert_apply(
        received, expert_gate, expert_up, expert_down, shared_gate_part, shared_up_part
    )
    returned = lax.all_to_all(results, "ep", split_axis=0, concat_axis=0, tiled=True)
    weight = jnp.where(select, dense_gate.T[:, None, :], zero_value)
    returned_rows = returned.reshape(experts_all, capacity, normed.shape[1]).astype(jnp.float32)
    routed = jnp.einsum("ect,ecd->td", weight, returned_rows, precision=lax.Precision.HIGHEST)
    shared_out = jnp.dot(shared_hidden, shared_down, preferred_element_type=jnp.float32)
    combined = routed + shared_out
    out_squares = lax.psum(jnp.sum(combined * combined, axis=1), "tp")
    return normalize(combined, out_gain, out_squares, D).astype(jnp.bfloat16)


F32 = jnp.float32
BF16 = jnp.bfloat16
LANES = 128


def flip(index, mask):
    out, bit = index, 1
    while bit <= mask:
        if mask & bit:
            out = out + bit - 2 * bit * ((index // bit) % 2)
        bit *= 2
    return out


def iota(shape, dim):
    return lax.broadcasted_iota(jnp.int32, shape, dim)


def dot(a, b):
    return jnp.dot(a, b, preferred_element_type=F32)


def batches(n_ep):
    far = list(range(2, n_ep, 2))
    return [[0], far[-2::-1], far[-1:]]


def fused_kernel(
    n_ep, n_tp, cap, width,
    tok_hbm, routes_hbm, gates_hbm, pre_hbm, eg_hbm, eu_hbm, ed_hbm, sg_hbm, su_hbm, sd_hbm, outg_hbm,
    o_ref,
    tok_ref, routes_ref, gates_ref, pre_ref, outg_ref,
    wg, wu, wd, sg, su, sd,
    xall, ss_all, bufs,
    rs_send, rs_recv, rsh_send, rsh_recv, rsh_own,
    hid_out, hid, hidsh, yown, yhold, ysend, ypair, zsend, zrecv, sq_all,
    w_sem, x_send, x_recv, ss_send, ss_recv, rs_ssem, rs_rsem, rsh_rsem,
    h_ssem, h_rsem, hs_rsem, p_ssem, p_rsem, y_rsem, q_ssem, q_rsem,
):
    me = lax.axis_index("ep")
    mine = lax.axis_index("tp")
    tok, dim = tok_ref.shape
    local = eg_hbm.shape[0]
    experts = local * n_ep
    top = routes_hbm.shape[0]
    part = eg_hbm.shape[2] // n_tp
    tp_masks = sorted(range(1, n_tp), key=lambda m: -bin(m).count("1"))
    evens = batches(n_ep)
    count = len(evens)
    order = [m for batch in evens for m in batch + [m + 1 for m in batch]]
    place = {m: i for i, m in enumerate(order)}
    owner = {m: b for b, batch in enumerate(evens) for m in batch}
    far = [m for batch in evens for m in batch if m]
    slot = {m: i for i, m in enumerate(far)}
    pairs = [len(batch) for batch in evens]
    start = [place[batch[0]] for batch in evens]
    span = [2 * p * tok for p in pairs]
    per = [2 * p * cap for p in pairs]
    rows = [local * p for p in per]

    def at_ep(mask):
        return {"ep": flip(me, mask)}

    def at_tp(mask):
        return {"tp": flip(mine, mask)}

    def across(mask):
        return {"ep": flip(me, 1), "tp": flip(mine, mask)}

    barrier = pltpu.get_barrier_semaphore()
    peers = [at_ep(m + 1) for m in [0] + far]
    peers += [where(m) for m in range(1, n_tp) for where in (at_tp, across)]
    for where in peers:
        pl.semaphore_signal(barrier, inc=1, device_id=where, device_id_type=pl.DeviceIdType.MESH)

    def columns(m):
        return pl.ds(pl.multiple_of(flip(mine, m) * part, part), part)

    copies = {}
    loads = (
        ("routes", routes_hbm, routes_ref), ("gates", gates_hbm, gates_ref), ("tok", tok_hbm, tok_ref),
        ("pre", pre_hbm, pre_ref),
    )
    for m in tp_masks + [0]:
        here = (slice(None), slice(None), columns(m))
        loads += ((("g", m), eg_hbm.at[here], wg.at[here]), (("u", m), eu_hbm.at[here], wu.at[here]))
    loads += (
        ("sg", sg_hbm, sg), ("su", su_hbm, su), ("sd", sd_hbm, sd), ("d", ed_hbm, wd), ("outg", outg_hbm, outg_ref),
    )
    for i, (name, src, dst) in enumerate(loads):
        copies[name] = pltpu.make_async_copy(src, dst, w_sem.at[i])
        if name not in ("sd", "d", "outg"):
            copies[name].start()

    def describe(src, dst, ssem, rsem, where):
        return pltpu.make_async_remote_copy(
            src_ref=src, dst_ref=dst, send_sem=ssem, recv_sem=rsem,
            device_id=where, device_id_type=pl.DeviceIdType.MESH,
        )

    def send(src, dst, ssem, rsem, where):
        describe(src, dst, ssem, rsem, where).start()

    def arrived(ref, ssem, rsem, where):
        describe(ref, ref, ssem, rsem, where).wait_recv()

    def sent(ref, ssem, rsem, where):
        describe(ref, ref, ssem, rsem, where).wait_send()

    def flat_gain(ref):
        value = ref[...].astype(F32)
        return jnp.concatenate([value[i : i + 1, :] for i in range(ref.shape[0])], axis=1)

    ss_all[:, 0] = jnp.zeros((ss_all.shape[0],) + ss_all.shape[2:], F32)
    for name in ("routes", "gates", "tok", "pre"):
        copies[name].wait()
    row = iota((LANES, tok), 0)
    names = row % experts
    dense = jnp.zeros((LANES, tok), F32)
    for k in range(top):
        dense = dense + jnp.where(routes_ref[k : k + 1, :] == names, gates_ref[k : k + 1, :], 0.0)
    earlier = jnp.where(iota((tok, tok), 0) < iota((tok, tok), 1), 1.0, 0.0).astype(BF16)
    slots = dot(jnp.where(dense > 0.0, 1.0, 0.0).astype(BF16), earlier)
    slots = jnp.where(dense > 0.0, slots + 1.0, 0.0)

    def terms(value):
        hi = value.astype(BF16).astype(F32)
        mid = (value - hi).astype(BF16).astype(F32)
        return hi, mid, value - hi - mid

    def choose(index, values):
        out = 0.0
        for i, value in enumerate(values):
            out = jnp.where(index == i, value, out)
        return out

    listed = choose(row // experts, terms(dense) + (slots,)).astype(BF16)
    eye = jnp.where(iota((tok, tok), 0) == iota((tok, tok), 1), 1.0, 0.0).astype(BF16)
    meta = lax.dot_general(eye, listed, (((1,), (1,)), ((), ())), preferred_element_type=F32)
    x = tok_ref[...].astype(F32)
    xall[0, :, :dim] = (x * flat_gain(pre_ref)).astype(BF16)
    squares = jnp.sum(x * x, axis=1, keepdims=True)
    lane = iota((tok, LANES), 1)
    meta = jnp.where(lane < 4 * experts, meta, choose(lane - 4 * experts, terms(squares)))
    xall[0, :, dim:] = meta.astype(BF16)

    pl.semaphore_wait(barrier, len(peers))

    def x_to(m, held, put, index):
        send(xall.at[held], xall.at[put], x_send.at[0], x_recv.at[index], at_ep(m))

    odd = len(far)
    x_to(1, 0, place[1], odd)
    for m in far[-2::-1] + far[-1:]:
        x_to(m + 1, 0, place[m + 1], slot[m])

    def relay(m):
        arrived(xall.at[place[m + 1]], x_send.at[0], x_recv.at[slot[m]], at_ep(m + 1))
        x_to(1, place[m + 1], place[m], odd + owner[m])

    xs = xall[0, :, :dim]
    def shared_piece(m):
        g = dot(xs, sg[:, columns(m)])
        u = dot(xs, su[:, columns(m)])
        if m:
            rsh_send[m - 1, :, :part] = g.astype(BF16)
            rsh_send[m - 1, :, part:] = u.astype(BF16)
            send(rsh_send.at[m - 1], rsh_recv.at[m - 1], rs_ssem.at[0], rsh_rsem.at[0], at_tp(m))
        else:
            rsh_own[:, :part] = g
            rsh_own[:, part:] = u

    def from_pair(b):
        return xall.at[pl.ds(start[b] if b else place[1], pairs[b])]

    row8, lane8 = iota((8, LANES), 0), iota((8, LANES), 1)
    gate_lane = lane8 < 3 * experts
    slot_lane = (lane8 >= 3 * experts) & (lane8 < 4 * experts)
    mine8 = me * local + row8
    pair8 = flip(me, 1) * local + row8
    pick = (
        ((row8 < local) & gate_lane & (lane8 % experts == mine8))
        | ((row8 == local) & (lane8 >= 4 * experts))
        | ((row8 > local) & (row8 <= 2 * local) & slot_lane & (lane8 % experts == mine8 - local - 1))
        | ((row8 > 2 * local) & (row8 <= 3 * local) & slot_lane & (lane8 % experts == pair8 - 2 * local - 1))
    )
    pick = jnp.where(pick, 1.0, 0.0).astype(BF16)
    tables, chosen, others, scale, own = {}, {}, {}, {}, {}

    def gather(b):
        arrived(from_pair(b), x_send.at[0], x_recv.at[odd + b], at_ep(1))
        blocks = pl.ds(start[b], 2 * pairs[b])
        tail = xall[blocks, :, dim:].reshape(span[b], LANES)
        table = lax.dot_general(pick, tail, (((1,), (1,)), ((), ())), preferred_element_type=F32)
        ss_all[b, 0, :, : span[b]] = table[local : local + 1, :]
        for m in tp_masks:
            send(ss_all.at[b, 0], ss_all.at[b, m], ss_send.at[0], ss_recv.at[b], at_tp(m))
        block = iota((8, span[b]), 1) // tok
        seen = (block + pairs[b]) % (2 * pairs[b])
        block = jnp.where(iota((8, span[b]), 0) > 2 * local, seen, block)
        target = jnp.where(table > 0.5, block * cap - 1 + table.astype(jnp.int32), -rows[b])

        def piece_of(e, base):
            goal = target[base + e : base + e + 1, :] + e * per[b]
            return jnp.where(iota((rows[b], span[b]), 0) == goal, 1.0, 0.0)

        pieces = [piece_of(e, local + 1) for e in range(local)]
        others[b] = sum(piece_of(e, 2 * local + 1) for e in range(local))
        tables[b], chosen[b] = table, pieces
        flat = xall[blocks, :, :dim].reshape(span[b], dim)
        for e in range(local):
            bufs[b][e] = dot(pieces[e].astype(BF16), flat).astype(BF16)

    def piece(b, m):
        if b == 0:
            copies["g", m].wait()
            copies["u", m].wait()
        g, u = 0.0, 0.0
        for e in range(local):
            rhs = bufs[b][e]
            g = g + dot(rhs, wg[e, :, columns(m)])
            u = u + dot(rhs, wu[e, :, columns(m)])
        rs_send[b][m, :, :part] = g.astype(BF16)
        rs_send[b][m, :, part:] = u.astype(BF16)
        send(rs_send[b].at[m], rs_recv[b].at[m], rs_ssem.at[0], rs_rsem.at[b], across(m))

    def scales(b):
        arrived(ss_all.at[b, pl.ds(1, n_tp - 1)], ss_send.at[0], ss_recv.at[b], at_tp(1))
        ss = ss_all[b, 0, :, : span[b]]
        for m in range(1, n_tp):
            ss = ss + ss_all[b, m, :, : span[b]]
        scale[b] = lax.rsqrt(ss / width + 1e-06)

    def activate(sums, by):
        g, u = sums[:, :part] * by, sums[:, part:] * by
        return (g / (1.0 + jnp.exp(-g)) * u).astype(BF16)

    def act(b):
        by = jnp.sum(others[b] * scale[b], axis=1, keepdims=True)
        arrived(rs_recv[b], rs_ssem.at[0], rs_rsem.at[b], across(1))
        sums = rs_recv[b][0].astype(F32)
        for m in tp_masks:
            sums = sums + rs_recv[b][m].astype(F32)
        hid_out[b][...] = activate(sums, by)
        for m in tp_masks:
            send(hid_out[b], hid[b].at[m], h_ssem.at[0], h_rsem.at[b * n_tp + m], across(m))
        send(hid_out[b], hid[b].at[0], h_ssem.at[0], h_rsem.at[b * n_tp], at_ep(1))

    def down(b, m, e, lo=0, hi=dim):
        depth = pl.ds(pl.multiple_of(flip(mine, m) * part, part), part)
        return dot(hid[b][m], wd[e, depth, lo:hi])

    def down_own(b):
        arrived(hid[b].at[0], h_ssem.at[0], h_rsem.at[b * n_tp], at_ep(1))
        own[b] = [down(b, 0, e) for e in range(local)]

    def down_near(b):
        for m in tp_masks[1:]:
            arrived(hid[b].at[m], h_ssem.at[0], h_rsem.at[b * n_tp + m], across(m))
            own[b] = [own[b][e] + down(b, m, e) for e in range(local)]

    def ypart(b):
        return pl.ds(start[b] // 2, pairs[b])

    def back(b, lo=0, hi=dim, index=0):
        m = tp_masks[0]
        if lo == 0:
            arrived(hid[b].at[m], h_ssem.at[0], h_rsem.at[b * n_tp + m], across(m))
        gated = 0.0
        for e in range(local):
            acc = own[b][e][:, lo:hi] + down(b, m, e, lo, hi)
            gated = gated + acc * jnp.sum(chosen[b][e] * tables[b][e : e + 1, :], axis=1, keepdims=True)
        y = lax.dot_general(
            sum(chosen[b]).astype(BF16), gated.astype(BF16), (((0,), (0,)), ((), ())), preferred_element_type=F32
        ).reshape(2 * pairs[b], tok, hi - lo)
        even, uneven = y[: pairs[b]], y[pairs[b] :]
        ysend[ypart(b), :, lo:hi] = (even if b else uneven).astype(BF16)
        yhold[ypart(b), :, lo:hi] = uneven if b else even
        block = (ypart(b), slice(None), pl.ds(lo, hi - lo))
        send(ysend.at[block], ypair.at[block], p_ssem.at[0], p_rsem.at[index], at_ep(1))

    def forward(b, lo=0, hi=dim, index=0):
        if b:
            block = (pl.ds(0, pairs[0] + pairs[1]) if b == 1 else ypart(b), slice(None), pl.ds(lo, hi - lo))
            arrived(ypair.at[block], p_ssem.at[0], p_rsem.at[index], at_ep(1))
        for i, m in enumerate(evens[b]):
            here = start[b] // 2 + i
            both = yhold[here, :, lo:hi] + ypair[here, :, lo:hi].astype(F32)
            if m:
                zsend[slot[m], :, lo:hi] = both.astype(BF16)
                block = (slot[m], slice(None), pl.ds(lo, hi - lo))
                send(zsend.at[block], zrecv.at[block], p_ssem.at[0], y_rsem.at[0], at_ep(m + 1))
            else:
                kept.append(both)

    def shared_act():
        match = jnp.where(iota((tok, span[0]), 1) == iota((tok, span[0]), 0), 1.0, 0.0)
        by = jnp.sum(match * scale[0], axis=1, keepdims=True)
        arrived(rsh_recv, rs_ssem.at[0], rsh_rsem.at[0], at_tp(1))
        sums = rsh_own[...]
        for m in tp_masks:
            sums = sums + rsh_recv[m - 1].astype(F32)
        hidsh[0] = activate(sums, by)
        for m in tp_masks:
            send(hidsh.at[0], hidsh.at[m], h_ssem.at[0], hs_rsem.at[0], at_tp(m))

    def shared_down():
        arrived(hidsh.at[pl.ds(1, n_tp - 1)], h_ssem.at[0], hs_rsem.at[0], at_tp(1))
        shared_out = 0.0
        for m in range(n_tp):
            depth = pl.ds(pl.multiple_of(flip(mine, m) * part, part), part)
            shared_out = shared_out + dot(hidsh[m], sd[depth, :])
        yown[...] = shared_out

    kept = []
    gather(0)
    for name in ("sd", "d", "outg"):
        copies[name].start()
    for m in tp_masks + [0]:
        piece(0, m)
    for m in evens[1]:
        relay(m)
    copies["sg"].wait()
    copies["su"].wait()
    for m in tp_masks + [0]:
        shared_piece(m)
    gather(1)
    piece(1, tp_masks[0])
    for m in evens[2]:
        relay(m)
    for m in tp_masks[1:]:
        piece(1, m)
    scales(0)
    act(0)
    gather(2)
    for m in tp_masks:
        piece(2, m)
    piece(1, 0)
    piece(2, 0)
    shared_act()
    copies["d"].wait()
    copies["sd"].wait()
    scales(1)
    act(1)
    scales(2)
    act(2)
    down_own(0)
    down_near(0)
    back(0)
    shared_down()
    down_own(1)
    down_own(2)
    down_near(1)
    back(1)
    down_near(2)
    back(2, 0, dim, 1)
    forward(1)
    forward(2, 0, dim, 1)
    forward(0)
    combined = yown[...]
    for both in kept:
        combined = combined + both
    copies["outg"].wait()
    arrived(zrecv, p_ssem.at[0], y_rsem.at[0], at_ep(3))
    for i in range(len(far)):
        combined = combined + zrecv[i].astype(F32)

    squared = combined * combined
    lanes = squared[:, :LANES]
    for c in range(LANES, dim, LANES):
        lanes = lanes + squared[:, c : c + LANES]
    sq_all[0] = lanes
    for m in tp_masks:
        send(sq_all.at[0], sq_all.at[m], q_ssem.at[0], q_rsem.at[0], at_tp(m))
    scaled = combined * flat_gain(outg_ref)
    arrived(sq_all.at[pl.ds(1, n_tp - 1)], q_ssem.at[0], q_rsem.at[0], at_tp(1))
    lanes = sq_all[0]
    for m in range(1, n_tp):
        lanes = lanes + sq_all[m]
    mean = jnp.sum(lanes, axis=1, keepdims=True) / width
    o_ref[...] = (scaled * lax.rsqrt(mean + 1e-06)).astype(BF16)
    sent(xall.at[pl.ds(0, n_ep - 1)], x_send.at[0], x_recv.at[0], at_ep(1))
    sent(ss_all.at[:, pl.ds(1, n_tp - 1)], ss_send.at[0], ss_recv.at[0], at_tp(1))
    lines = n_tp * sum(rows) + (n_tp - 1) * tok
    sent(wd.at[0, pl.ds(0, lines), pl.ds(0, 2 * part)], rs_ssem.at[0], rs_rsem.at[0], across(1))
    sent(wd.at[0, pl.ds(0, lines), pl.ds(0, part)], h_ssem.at[0], h_rsem.at[0], across(1))
    sent(wd.at[0, pl.ds(0, (sum(pairs) + len(far)) * tok), :], p_ssem.at[0], p_rsem.at[0], at_ep(1))
    sent(sq_all.at[pl.ds(1, n_tp - 1)], q_ssem.at[0], q_rsem.at[0], at_tp(1))


def fused(n_ep, n_tp, tokens, routes, gates, pre_gain, eg, eu, ed, sg, su, sd, out_gain):
    tok, dim = tokens.shape
    local, _, hidden = eg.shape
    top = routes.shape[1]
    cap = max(2, 3 * tok * top // (2 * local * n_ep))
    half = n_ep // 2
    evens = batches(n_ep)
    count = len(evens)
    rows = [local * 2 * len(batch) * cap for batch in evens]
    part = hidden // n_tp
    anywhere = pl.BlockSpec(memory_space=pl.ANY)
    sems = lambda n: pltpu.SemaphoreType.DMA((n,))
    return pl.pallas_call(
        functools.partial(fused_kernel, n_ep, n_tp, cap, dim * n_tp),
        out_shape=pltpu.VMEM((tok, dim), BF16),
        in_specs=[anywhere] * 11,
        out_specs=pl.BlockSpec(memory_space=pltpu.VMEM),
        scratch_shapes=[
            pltpu.VMEM((tok, dim), BF16), pltpu.VMEM((top, tok), jnp.int32), pltpu.VMEM((top, tok), F32),
            pltpu.VMEM((dim // LANES, LANES), BF16), pltpu.VMEM((dim // LANES, LANES), BF16),
            pltpu.VMEM(eg.shape, BF16), pltpu.VMEM(eu.shape, BF16), pltpu.VMEM(ed.shape, BF16),
            pltpu.VMEM(sg.shape, BF16), pltpu.VMEM(su.shape, BF16), pltpu.VMEM(sd.shape, BF16),
            pltpu.VMEM((n_ep, tok, dim + LANES), BF16),
            pltpu.VMEM((count, n_tp, 1, LANES), F32),
            [pltpu.VMEM((local, r, dim), BF16) for r in rows],
            [pltpu.VMEM((n_tp, r, 2 * part), BF16) for r in rows],
            [pltpu.VMEM((n_tp, r, 2 * part), BF16) for r in rows],
            pltpu.VMEM((n_tp - 1, tok, 2 * part), BF16),
            pltpu.VMEM((n_tp - 1, tok, 2 * part), BF16),
            pltpu.VMEM((tok, 2 * part), F32),
            [pltpu.VMEM((r, part), BF16) for r in rows],
            [pltpu.VMEM((n_tp, r, part), BF16) for r in rows],
            pltpu.VMEM((n_tp, tok, part), BF16),
            pltpu.VMEM((tok, dim), F32),
            pltpu.VMEM((half, tok, dim), F32),
            pltpu.VMEM((half, tok, dim), BF16),
            pltpu.VMEM((half, tok, dim), BF16),
            pltpu.VMEM((half - 1, tok, dim), BF16),
            pltpu.VMEM((half - 1, tok, dim), BF16),
            pltpu.VMEM((n_tp, tok, LANES), F32),
            sems(9 + 2 * n_tp),
            sems(1), sems(half - 1 + count), sems(1), sems(count), sems(1), sems(count), sems(1),
            sems(1), sems(n_tp * count), sems(1), sems(1), sems(3), sems(1), sems(1), sems(1),
        ],
        compiler_params=pltpu.CompilerParams(
            collective_id=0, has_side_effects=True, vmem_limit_bytes=60 * 1024 * 1024
        ),
    )(
        tokens, routes.T, gates.T, pre_gain.reshape(-1, LANES), eg, eu, ed, sg, su, sd,
        out_gain.reshape(-1, LANES),
    )


def fits(n_ep, n_tp, tokens, routes, eg):
    tok, dim = tokens.shape
    local, _, hidden = eg.shape
    experts = local * n_ep
    cap = max(2, 3 * tok * routes.shape[1] // (2 * experts))
    power = (n_ep & (n_ep - 1)) == 0 and (n_tp & (n_tp - 1)) == 0
    return (
        power
        and n_ep > 4
        and n_tp > 1
        and hidden % (LANES * n_tp) == 0
        and dim % LANES == 0
        and tok % 16 == 0
        and n_ep * tok == LANES
        and 4 * experts + 3 <= LANES
        and 3 * local < 8
    )


def per_device(*args):
    n_ep, n_tp = lax.axis_size("ep"), lax.axis_size("tp")
    if fits(n_ep, n_tp, args[0], args[1], args[4]):
        return fused(n_ep, n_tp, *args)
    return on_device(*args)


def solution(mesh):
    in_specs = (
        P("ep", "tp"),
        P("ep", None),
        P("ep", None),
        P("tp"),
        P("ep", "tp", None),
        P("ep", "tp", None),
        P("ep", None, "tp"),
        P("tp", None),
        P("tp", None),
        P(None, "tp"),
        P("tp"),
    )
    out_specs = P("ep", "tp")
    return jax.shard_map(
        per_device, mesh=mesh, in_specs=in_specs, out_specs=out_specs, check_vma=False
    )
```

```python
import functools
import jax
import jax.numpy as jnp
from jax import lax
from jax.experimental import pallas as pl
from jax.experimental.pallas import tpu as pltpu
from jax.sharding import PartitionSpec as P

D = 4096


def normalize(values, gain, squares, width):
    scale = lax.rsqrt(squares[:, None] / width + 1e-06)
    return values * scale * gain.astype(jnp.float32)


def expert_apply(buffer, expert_gate, expert_up, expert_down, shared_gate_part, shared_up_part):
    gate_part = jnp.einsum(
        "secd,edf->secf", buffer, expert_gate, preferred_element_type=jnp.float32
    )
    up_part = jnp.einsum("secd,edf->secf", buffer, expert_up, preferred_element_type=jnp.float32)
    gate_act, up_act, shared_gate_act, shared_up_act = lax.psum(
        (gate_part, up_part, shared_gate_part, shared_up_part), "tp"
    )
    hidden = (jax.nn.silu(gate_act) * up_act).astype(jnp.bfloat16)
    shared_hidden = (jax.nn.silu(shared_gate_act) * shared_up_act).astype(jnp.bfloat16)
    results = jnp.einsum(
        "secf,efd->secd", hidden, expert_down, preferred_element_type=jnp.float32
    ).astype(jnp.bfloat16)
    return (results, shared_hidden)


def on_device(
    tokens,
    routes,
    gates,
    pre_gain,
    expert_gate,
    expert_up,
    expert_down,
    shared_gate,
    shared_up,
    shared_down,
    out_gain,
):
    own_rows = tokens.astype(jnp.float32)
    in_squares = lax.psum(jnp.sum(own_rows * own_rows, axis=1), "tp")
    normed = normalize(own_rows, pre_gain, in_squares, D).astype(jnp.bfloat16)
    shared_gate_part = jnp.dot(normed, shared_gate, preferred_element_type=jnp.float32)
    shared_up_part = jnp.dot(normed, shared_up, preferred_element_type=jnp.float32)
    tok_count = tokens.shape[0]
    top_count = routes.shape[1]
    groups = lax.axis_size("ep")
    local_experts = expert_gate.shape[0]
    experts_all = local_experts * groups
    capacity = max(2, 3 * tok_count * top_count // (2 * experts_all))
    places = jnp.arange(capacity, dtype=jnp.int32)
    zero_value = jnp.zeros((), jnp.float32)
    labels = jnp.arange(experts_all, dtype=jnp.int32)
    picked = routes[:, :, None] == labels[None, None, :]
    onehot = jnp.sum(picked.astype(jnp.int32), axis=1)
    dense_gate = jnp.sum(jnp.where(picked, gates[:, :, None], zero_value), axis=1)
    slot_index = jnp.cumsum(onehot, axis=0) - onehot
    select = (slot_index.T[:, None, :] == places[None, :, None]) & (onehot.T[:, None, :] > 0)
    outgoing = jnp.einsum(
        "ect,td->ecd", select.astype(jnp.bfloat16), normed, preferred_element_type=jnp.float32
    ).astype(jnp.bfloat16)
    outgoing = outgoing.reshape(groups, local_experts, capacity, normed.shape[1])
    received = lax.all_to_all(outgoing, "ep", split_axis=0, concat_axis=0, tiled=True)
    results, shared_hidden = expert_apply(
        received, expert_gate, expert_up, expert_down, shared_gate_part, shared_up_part
    )
    returned = lax.all_to_all(results, "ep", split_axis=0, concat_axis=0, tiled=True)
    weight = jnp.where(select, dense_gate.T[:, None, :], zero_value)
    returned_rows = returned.reshape(experts_all, capacity, normed.shape[1]).astype(jnp.float32)
    routed = jnp.einsum("ect,ecd->td", weight, returned_rows, precision=lax.Precision.HIGHEST)
    shared_out = jnp.dot(shared_hidden, shared_down, preferred_element_type=jnp.float32)
    combined = routed + shared_out
    out_squares = lax.psum(jnp.sum(combined * combined, axis=1), "tp")
    return normalize(combined, out_gain, out_squares, D).astype(jnp.bfloat16)


F32 = jnp.float32
BF16 = jnp.bfloat16
LANES = 128


def flip(index, mask):
    out, bit = index, 1
    while bit <= mask:
        if mask & bit:
            out = out + bit - 2 * bit * ((index // bit) % 2)
        bit *= 2
    return out


def iota(shape, dim):
    return lax.broadcasted_iota(jnp.int32, shape, dim)


def dot(a, b):
    return jnp.dot(a, b, preferred_element_type=F32)


def batches(n_ep):
    far = list(range(2, n_ep, 2))
    return [[0], far[-2::-1], far[-1:]]


def fused_kernel(
    n_ep, n_tp, cap, width,
    tok_hbm, routes_hbm, gates_hbm, pre_hbm, eg_hbm, eu_hbm, ed_hbm, sg_hbm, su_hbm, sd_hbm, outg_hbm,
    o_ref,
    tok_ref, routes_ref, gates_ref, pre_ref, outg_ref,
    wg, wu, wd, sg, su, sd,
    xall, ss_all, bufs,
    rs_send, rs_recv, rsh_send, rsh_recv, rsh_own,
    hid_out, hid, hidsh, yown, yhold, ysend, ypair, zsend, zrecv, sq_all,
    w_sem, x_send, x_recv, ss_send, ss_recv, rs_ssem, rs_rsem, rsh_rsem,
    h_ssem, h_rsem, hs_rsem, p_ssem, p_rsem, y_rsem, q_ssem, q_rsem,
):
    me = lax.axis_index("ep")
    mine = lax.axis_index("tp")
    tok, dim = tok_ref.shape
    local = eg_hbm.shape[0]
    experts = local * n_ep
    top = routes_hbm.shape[0]
    part = eg_hbm.shape[2] // n_tp
    tp_masks = sorted(range(1, n_tp), key=lambda m: -bin(m).count("1"))
    evens = batches(n_ep)
    count = len(evens)
    order = [m for batch in evens for m in batch + [m + 1 for m in batch]]
    place = {m: i for i, m in enumerate(order)}
    owner = {m: b for b, batch in enumerate(evens) for m in batch}
    far = [m for batch in evens for m in batch if m]
    slot = {m: i for i, m in enumerate(far)}
    pairs = [len(batch) for batch in evens]
    start = [place[batch[0]] for batch in evens]
    span = [2 * p * tok for p in pairs]
    per = [2 * p * cap for p in pairs]
    rows = [local * p for p in per]

    def at_ep(mask):
        return {"ep": flip(me, mask)}

    def at_tp(mask):
        return {"tp": flip(mine, mask)}

    def across(mask):
        return {"ep": flip(me, 1), "tp": flip(mine, mask)}

    barrier = pltpu.get_barrier_semaphore()
    peers = [at_ep(m + 1) for m in [0] + far]
    peers += [where(m) for m in range(1, n_tp) for where in (at_tp, across)]
    for where in peers:
        pl.semaphore_signal(barrier, inc=1, device_id=where, device_id_type=pl.DeviceIdType.MESH)

    def columns(m):
        return pl.ds(pl.multiple_of(flip(mine, m) * part, part), part)

    copies = {}
    loads = (
        ("routes", routes_hbm, routes_ref), ("gates", gates_hbm, gates_ref), ("tok", tok_hbm, tok_ref),
        ("pre", pre_hbm, pre_ref),
    )
    for m in tp_masks + [0]:
        here = (slice(None), slice(None), columns(m))
        loads += ((("g", m), eg_hbm.at[here], wg.at[here]), (("u", m), eu_hbm.at[here], wu.at[here]))
    loads += (
        ("sg", sg_hbm, sg), ("su", su_hbm, su), ("sd", sd_hbm, sd), ("d", ed_hbm, wd), ("outg", outg_hbm, outg_ref),
    )
    for i, (name, src, dst) in enumerate(loads):
        copies[name] = pltpu.make_async_copy(src, dst, w_sem.at[i])
        if name not in ("sd", "d", "outg"):
            copies[name].start()

    def describe(src, dst, ssem, rsem, where):
        return pltpu.make_async_remote_copy(
            src_ref=src, dst_ref=dst, send_sem=ssem, recv_sem=rsem,
            device_id=where, device_id_type=pl.DeviceIdType.MESH,
        )

    def send(src, dst, ssem, rsem, where):
        describe(src, dst, ssem, rsem, where).start()

    def arrived(ref, ssem, rsem, where):
        describe(ref, ref, ssem, rsem, where).wait_recv()

    def sent(ref, ssem, rsem, where):
        describe(ref, ref, ssem, rsem, where).wait_send()

    def flat_gain(ref):
        value = ref[...].astype(F32)
        return jnp.concatenate([value[i : i + 1, :] for i in range(ref.shape[0])], axis=1)

    ss_all[:, 0] = jnp.zeros((ss_all.shape[0],) + ss_all.shape[2:], F32)
    for name in ("routes", "gates", "tok", "pre"):
        copies[name].wait()
    row = iota((LANES, tok), 0)
    names = row % experts
    dense = jnp.zeros((LANES, tok), F32)
    for k in range(top):
        dense = dense + jnp.where(routes_ref[k : k + 1, :] == names, gates_ref[k : k + 1, :], 0.0)
    named = jnp.where(dense > 0.0, 1.0, 0.0)

    def terms(value):
        hi = value.astype(BF16).astype(F32)
        mid = (value - hi).astype(BF16).astype(F32)
        return hi, mid, value - hi - mid

    def choose(index, values):
        out = 0.0
        for i, value in enumerate(values):
            out = jnp.where(index == i, value, out)
        return out

    def flipped(left, right):
        return lax.dot_general(
            jnp.where(left, 1.0, 0.0).astype(BF16), right.astype(BF16), (((1,), (1,)), ((), ())),
            preferred_element_type=F32,
        )

    here, there = iota((tok, tok), 0), iota((tok, tok), 1)
    meta = flipped(here == there, choose(row // experts, terms(dense) + (named,)))
    before = flipped(there < here, named)
    x = tok_ref[...].astype(F32)
    xall[0, :, :dim] = (x * flat_gain(pre_ref)).astype(BF16)
    squares = jnp.sum(x * x, axis=1, keepdims=True)
    lane = iota((tok, LANES), 1)
    meta = jnp.where(lane < 3 * experts, meta, meta * (before + 1.0))
    meta = jnp.where(lane < 4 * experts, meta, choose(lane - 4 * experts, terms(squares)))
    xall[0, :, dim:] = meta.astype(BF16)

    pl.semaphore_wait(barrier, len(peers))

    def x_to(m, held, put, index):
        send(xall.at[held], xall.at[put], x_send.at[0], x_recv.at[index], at_ep(m))

    odd = len(far)
    x_to(1, 0, place[1], odd)
    for m in far[-2::-1] + far[-1:]:
        x_to(m + 1, 0, place[m + 1], slot[m])

    def relay(m):
        arrived(xall.at[place[m + 1]], x_send.at[0], x_recv.at[slot[m]], at_ep(m + 1))
        x_to(1, place[m + 1], place[m], odd + owner[m])

    xs = xall[0, :, :dim]
    def shared_piece(m):
        g = dot(xs, sg[:, columns(m)])
        u = dot(xs, su[:, columns(m)])
        if m:
            rsh_send[m - 1, :, :part] = g.astype(BF16)
            rsh_send[m - 1, :, part:] = u.astype(BF16)
            send(rsh_send.at[m - 1], rsh_recv.at[m - 1], rs_ssem.at[0], rsh_rsem.at[0], at_tp(m))
        else:
            rsh_own[:, :part] = g
            rsh_own[:, part:] = u

    def from_pair(b):
        return xall.at[pl.ds(start[b] if b else place[1], pairs[b])]

    row8, lane8 = iota((8, LANES), 0), iota((8, LANES), 1)
    gate_lane = lane8 < 3 * experts
    slot_lane = (lane8 >= 3 * experts) & (lane8 < 4 * experts)
    mine8 = me * local + row8
    pair8 = flip(me, 1) * local + row8
    pick = (
        ((row8 < local) & gate_lane & (lane8 % experts == mine8))
        | ((row8 == local) & (lane8 >= 4 * experts))
        | ((row8 > local) & (row8 <= 2 * local) & slot_lane & (lane8 % experts == mine8 - local - 1))
        | ((row8 > 2 * local) & (row8 <= 3 * local) & slot_lane & (lane8 % experts == pair8 - 2 * local - 1))
    )
    pick = jnp.where(pick, 1.0, 0.0).astype(BF16)
    tables, chosen, others, scale, own = {}, {}, {}, {}, {}

    def gather(b):
        arrived(from_pair(b), x_send.at[0], x_recv.at[odd + b], at_ep(1))
        blocks = pl.ds(start[b], 2 * pairs[b])
        tail = xall[blocks, :, dim:].reshape(span[b], LANES)
        table = lax.dot_general(pick, tail, (((1,), (1,)), ((), ())), preferred_element_type=F32)
        ss_all[b, 0, :, : span[b]] = table[local : local + 1, :]
        for m in tp_masks:
            send(ss_all.at[b, 0], ss_all.at[b, m], ss_send.at[0], ss_recv.at[b], at_tp(m))
        block = iota((8, span[b]), 1) // tok
        seen = (block + pairs[b]) % (2 * pairs[b])
        block = jnp.where(iota((8, span[b]), 0) > 2 * local, seen, block)
        target = jnp.where(table > 0.5, block * cap - 1 + table.astype(jnp.int32), -rows[b])

        def piece_of(e, base):
            goal = target[base + e : base + e + 1, :] + e * per[b]
            return jnp.where(iota((rows[b], span[b]), 0) == goal, 1.0, 0.0)

        pieces = [piece_of(e, local + 1) for e in range(local)]
        others[b] = sum(piece_of(e, 2 * local + 1) for e in range(local))
        tables[b], chosen[b] = table, pieces
        flat = xall[blocks, :, :dim].reshape(span[b], dim)
        for e in range(local):
            bufs[b][e] = dot(pieces[e].astype(BF16), flat).astype(BF16)

    def piece(b, m):
        if b == 0:
            copies["g", m].wait()
            copies["u", m].wait()
        g, u = 0.0, 0.0
        for e in range(local):
            rhs = bufs[b][e]
            g = g + dot(rhs, wg[e, :, columns(m)])
            u = u + dot(rhs, wu[e, :, columns(m)])
        rs_send[b][m, :, :part] = g.astype(BF16)
        rs_send[b][m, :, part:] = u.astype(BF16)
        send(rs_send[b].at[m], rs_recv[b].at[m], rs_ssem.at[0], rs_rsem.at[b], across(m))

    def scales(b):
        arrived(ss_all.at[b, pl.ds(1, n_tp - 1)], ss_send.at[0], ss_recv.at[b], at_tp(1))
        ss = ss_all[b, 0, :, : span[b]]
        for m in range(1, n_tp):
            ss = ss + ss_all[b, m, :, : span[b]]
        scale[b] = lax.rsqrt(ss / width + 1e-06)

    def activate(sums, by):
        g, u = sums[:, :part] * by, sums[:, part:] * by
        return (g / (1.0 + jnp.exp(-g)) * u).astype(BF16)

    def hidden_at(b, m):
        return 1 + (b - 1) * n_tp + m if b else 0

    def act(b):
        by = jnp.sum(others[b] * scale[b], axis=1, keepdims=True)
        arrived(rs_recv[b], rs_ssem.at[0], rs_rsem.at[b], across(1))
        sums = rs_recv[b][0].astype(F32)
        for m in tp_masks:
            sums = sums + rs_recv[b][m].astype(F32)
        hid_out[b][...] = activate(sums, by)
        for m in tp_masks:
            send(hid_out[b], hid[b].at[m], h_ssem.at[0], h_rsem.at[hidden_at(b, m)], across(m))
        send(hid_out[b], hid[b].at[0], h_ssem.at[0], h_rsem.at[hidden_at(b, 0)], at_ep(1))

    def down(b, m, e, lo=0, hi=dim):
        depth = pl.ds(pl.multiple_of(flip(mine, m) * part, part), part)
        return dot(hid[b][m], wd[e, depth, lo:hi])

    def down_own(b):
        arrived(hid[b].at[0] if b else hid[b], h_ssem.at[0], h_rsem.at[hidden_at(b, 0)], at_ep(1))
        own[b] = [down(b, 0, e) for e in range(local)]

    def down_near(b):
        for m in tp_masks[1:]:
            if b:
                arrived(hid[b].at[m], h_ssem.at[0], h_rsem.at[hidden_at(b, m)], across(m))
            own[b] = [own[b][e] + down(b, m, e) for e in range(local)]

    def ypart(b):
        return pl.ds(start[b] // 2, pairs[b])

    def back(b, lo=0, hi=dim, index=0):
        m = tp_masks[0]
        if b and lo == 0:
            arrived(hid[b].at[m], h_ssem.at[0], h_rsem.at[hidden_at(b, m)], across(m))
        gated = 0.0
        for e in range(local):
            acc = own[b][e][:, lo:hi] + down(b, m, e, lo, hi)
            gated = gated + acc * jnp.sum(chosen[b][e] * tables[b][e : e + 1, :], axis=1, keepdims=True)
        y = lax.dot_general(
            sum(chosen[b]).astype(BF16), gated.astype(BF16), (((0,), (0,)), ((), ())), preferred_element_type=F32
        ).reshape(2 * pairs[b], tok, hi - lo)
        even, uneven = y[: pairs[b]], y[pairs[b] :]
        ysend[ypart(b), :, lo:hi] = (even if b else uneven).astype(BF16)
        yhold[ypart(b), :, lo:hi] = uneven if b else even
        block = (ypart(b), slice(None), pl.ds(lo, hi - lo))
        send(ysend.at[block], ypair.at[block], p_ssem.at[0], p_rsem.at[index], at_ep(1))

    def forward(b, lo=0, hi=dim, index=0):
        if b:
            block = (pl.ds(0, pairs[0] + pairs[1]) if b == 1 else ypart(b), slice(None), pl.ds(lo, hi - lo))
            arrived(ypair.at[block], p_ssem.at[0], p_rsem.at[index], at_ep(1))
        for i, m in enumerate(evens[b]):
            here = start[b] // 2 + i
            both = yhold[here, :, lo:hi] + ypair[here, :, lo:hi].astype(F32)
            if m:
                zsend[slot[m], :, lo:hi] = both.astype(BF16)
                block = (slot[m], slice(None), pl.ds(lo, hi - lo))
                send(zsend.at[block], zrecv.at[block], p_ssem.at[0], y_rsem.at[0], at_ep(m + 1))
            else:
                kept.append(both)

    def shared_act():
        match = jnp.where(iota((tok, span[0]), 1) == iota((tok, span[0]), 0), 1.0, 0.0)
        by = jnp.sum(match * scale[0], axis=1, keepdims=True)
        arrived(rsh_recv, rs_ssem.at[0], rsh_rsem.at[0], at_tp(1))
        sums = rsh_own[...]
        for m in tp_masks:
            sums = sums + rsh_recv[m - 1].astype(F32)
        hidsh[0] = activate(sums, by)
        for m in tp_masks:
            send(hidsh.at[0], hidsh.at[m], h_ssem.at[0], hs_rsem.at[0], at_tp(m))

    def shared_down():
        arrived(hidsh.at[pl.ds(1, n_tp - 1)], h_ssem.at[0], hs_rsem.at[0], at_tp(1))
        shared_out = 0.0
        for m in range(n_tp):
            depth = pl.ds(pl.multiple_of(flip(mine, m) * part, part), part)
            shared_out = shared_out + dot(hidsh[m], sd[depth, :])
        yown[...] = shared_out

    kept = []
    gather(0)
    for name in ("sd", "d", "outg"):
        copies[name].start()
    for m in tp_masks + [0]:
        piece(0, m)
    for m in evens[1]:
        relay(m)
    copies["sg"].wait()
    copies["su"].wait()
    for m in tp_masks + [0]:
        shared_piece(m)
    gather(1)
    piece(1, tp_masks[0])
    for m in evens[2]:
        relay(m)
    for m in tp_masks[1:]:
        piece(1, m)
    scales(0)
    act(0)
    gather(2)
    for m in tp_masks:
        piece(2, m)
    piece(1, 0)
    piece(2, 0)
    shared_act()
    copies["d"].wait()
    copies["sd"].wait()
    scales(1)
    act(1)
    scales(2)
    act(2)
    down_own(0)
    down_near(0)
    back(0)
    shared_down()
    down_own(1)
    down_own(2)
    down_near(1)
    back(1)
    down_near(2)
    back(2, 0, dim, 1)
    forward(1)
    forward(2, 0, dim, 1)
    forward(0)
    combined = yown[...]
    for both in kept:
        combined = combined + both
    copies["outg"].wait()
    arrived(zrecv, p_ssem.at[0], y_rsem.at[0], at_ep(3))
    for i in range(len(far)):
        combined = combined + zrecv[i].astype(F32)

    squared = combined * combined
    lanes = squared[:, :LANES]
    for c in range(LANES, dim, LANES):
        lanes = lanes + squared[:, c : c + LANES]
    sq_all[0] = lanes
    for m in tp_masks:
        send(sq_all.at[0], sq_all.at[m], q_ssem.at[0], q_rsem.at[0], at_tp(m))
    scaled = combined * flat_gain(outg_ref)
    arrived(sq_all.at[pl.ds(1, n_tp - 1)], q_ssem.at[0], q_rsem.at[0], at_tp(1))
    lanes = sq_all[0]
    for m in range(1, n_tp):
        lanes = lanes + sq_all[m]
    mean = jnp.sum(lanes, axis=1, keepdims=True) / width
    o_ref[...] = (scaled * lax.rsqrt(mean + 1e-06)).astype(BF16)
    sent(xall.at[pl.ds(0, n_ep - 1)], x_send.at[0], x_recv.at[0], at_ep(1))
    sent(ss_all.at[:, pl.ds(1, n_tp - 1)], ss_send.at[0], ss_recv.at[0], at_tp(1))
    lines = n_tp * sum(rows) + (n_tp - 1) * tok
    sent(wd.at[0, pl.ds(0, lines), pl.ds(0, 2 * part)], rs_ssem.at[0], rs_rsem.at[0], across(1))
    sent(wd.at[0, pl.ds(0, lines), pl.ds(0, part)], h_ssem.at[0], h_rsem.at[0], across(1))
    sent(wd.at[0, pl.ds(0, (sum(pairs) + len(far)) * tok), :], p_ssem.at[0], p_rsem.at[0], at_ep(1))
    sent(sq_all.at[pl.ds(1, n_tp - 1)], q_ssem.at[0], q_rsem.at[0], at_tp(1))


def fused(n_ep, n_tp, tokens, routes, gates, pre_gain, eg, eu, ed, sg, su, sd, out_gain):
    tok, dim = tokens.shape
    local, _, hidden = eg.shape
    top = routes.shape[1]
    cap = max(2, 3 * tok * top // (2 * local * n_ep))
    half = n_ep // 2
    evens = batches(n_ep)
    count = len(evens)
    rows = [local * 2 * len(batch) * cap for batch in evens]
    part = hidden // n_tp
    anywhere = pl.BlockSpec(memory_space=pl.ANY)
    sems = lambda n: pltpu.SemaphoreType.DMA((n,))
    return pl.pallas_call(
        functools.partial(fused_kernel, n_ep, n_tp, cap, dim * n_tp),
        out_shape=pltpu.VMEM((tok, dim), BF16),
        in_specs=[anywhere] * 11,
        out_specs=pl.BlockSpec(memory_space=pltpu.VMEM),
        scratch_shapes=[
            pltpu.VMEM((tok, dim), BF16), pltpu.VMEM((top, tok), jnp.int32), pltpu.VMEM((top, tok), F32),
            pltpu.VMEM((dim // LANES, LANES), BF16), pltpu.VMEM((dim // LANES, LANES), BF16),
            pltpu.VMEM(eg.shape, BF16), pltpu.VMEM(eu.shape, BF16), pltpu.VMEM(ed.shape, BF16),
            pltpu.VMEM(sg.shape, BF16), pltpu.VMEM(su.shape, BF16), pltpu.VMEM(sd.shape, BF16),
            pltpu.VMEM((n_ep, tok, dim + LANES), BF16),
            pltpu.VMEM((count, n_tp, 1, LANES), F32),
            [pltpu.VMEM((local, r, dim), BF16) for r in rows],
            [pltpu.VMEM((n_tp, r, 2 * part), BF16) for r in rows],
            [pltpu.VMEM((n_tp, r, 2 * part), BF16) for r in rows],
            pltpu.VMEM((n_tp - 1, tok, 2 * part), BF16),
            pltpu.VMEM((n_tp - 1, tok, 2 * part), BF16),
            pltpu.VMEM((tok, 2 * part), F32),
            [pltpu.VMEM((r, part), BF16) for r in rows],
            [pltpu.VMEM((n_tp, r, part), BF16) for r in rows],
            pltpu.VMEM((n_tp, tok, part), BF16),
            pltpu.VMEM((tok, dim), F32),
            pltpu.VMEM((half, tok, dim), F32),
            pltpu.VMEM((half, tok, dim), BF16),
            pltpu.VMEM((half, tok, dim), BF16),
            pltpu.VMEM((half - 1, tok, dim), BF16),
            pltpu.VMEM((half - 1, tok, dim), BF16),
            pltpu.VMEM((n_tp, tok, LANES), F32),
            sems(9 + 2 * n_tp),
            sems(1), sems(half - 1 + count), sems(1), sems(count), sems(1), sems(count), sems(1),
            sems(1), sems(1 + n_tp * (count - 1)), sems(1), sems(1), sems(2), sems(1), sems(1), sems(1),
        ],
        compiler_params=pltpu.CompilerParams(
            collective_id=0, has_side_effects=True, vmem_limit_bytes=60 * 1024 * 1024
        ),
    )(
        tokens, routes.T, gates.T, pre_gain.reshape(-1, LANES), eg, eu, ed, sg, su, sd,
        out_gain.reshape(-1, LANES),
    )


def fits(n_ep, n_tp, tokens, routes, eg):
    tok, dim = tokens.shape
    local, _, hidden = eg.shape
    experts = local * n_ep
    cap = max(2, 3 * tok * routes.shape[1] // (2 * experts))
    power = (n_ep & (n_ep - 1)) == 0 and (n_tp & (n_tp - 1)) == 0
    return (
        power
        and n_ep > 4
        and n_tp > 1
        and hidden % (LANES * n_tp) == 0
        and dim % LANES == 0
        and tok % 16 == 0
        and n_ep * tok == LANES
        and 4 * experts + 3 <= LANES
        and 3 * local < 8
    )


def per_device(*args):
    n_ep, n_tp = lax.axis_size("ep"), lax.axis_size("tp")
    if fits(n_ep, n_tp, args[0], args[1], args[4]):
        return fused(n_ep, n_tp, *args)
    return on_device(*args)


def solution(mesh):
    in_specs = (
        P("ep", "tp"),
        P("ep", None),
        P("ep", None),
        P("tp"),
        P("ep", "tp", None),
        P("ep", "tp", None),
        P("ep", None, "tp"),
        P("tp", None),
        P("tp", None),
        P(None, "tp"),
        P("tp"),
    )
    out_specs = P("ep", "tp")
    return jax.shard_map(
        per_device, mesh=mesh, in_specs=in_specs, out_specs=out_specs, check_vma=False
    )
```

```python
import functools
import jax
import jax.numpy as jnp
from jax import lax
from jax.experimental import pallas as pl
from jax.experimental.pallas import tpu as pltpu
from jax.sharding import PartitionSpec as P

D = 4096


def normalize(values, gain, squares, width):
    scale = lax.rsqrt(squares[:, None] / width + 1e-06)
    return values * scale * gain.astype(jnp.float32)


def expert_apply(buffer, expert_gate, expert_up, expert_down, shared_gate_part, shared_up_part):
    gate_part = jnp.einsum(
        "secd,edf->secf", buffer, expert_gate, preferred_element_type=jnp.float32
    )
    up_part = jnp.einsum("secd,edf->secf", buffer, expert_up, preferred_element_type=jnp.float32)
    gate_act, up_act, shared_gate_act, shared_up_act = lax.psum(
        (gate_part, up_part, shared_gate_part, shared_up_part), "tp"
    )
    hidden = (jax.nn.silu(gate_act) * up_act).astype(jnp.bfloat16)
    shared_hidden = (jax.nn.silu(shared_gate_act) * shared_up_act).astype(jnp.bfloat16)
    results = jnp.einsum(
        "secf,efd->secd", hidden, expert_down, preferred_element_type=jnp.float32
    ).astype(jnp.bfloat16)
    return (results, shared_hidden)


def on_device(
    tokens,
    routes,
    gates,
    pre_gain,
    expert_gate,
    expert_up,
    expert_down,
    shared_gate,
    shared_up,
    shared_down,
    out_gain,
):
    own_rows = tokens.astype(jnp.float32)
    in_squares = lax.psum(jnp.sum(own_rows * own_rows, axis=1), "tp")
    normed = normalize(own_rows, pre_gain, in_squares, D).astype(jnp.bfloat16)
    shared_gate_part = jnp.dot(normed, shared_gate, preferred_element_type=jnp.float32)
    shared_up_part = jnp.dot(normed, shared_up, preferred_element_type=jnp.float32)
    tok_count = tokens.shape[0]
    top_count = routes.shape[1]
    groups = lax.axis_size("ep")
    local_experts = expert_gate.shape[0]
    experts_all = local_experts * groups
    capacity = max(2, 3 * tok_count * top_count // (2 * experts_all))
    places = jnp.arange(capacity, dtype=jnp.int32)
    zero_value = jnp.zeros((), jnp.float32)
    labels = jnp.arange(experts_all, dtype=jnp.int32)
    picked = routes[:, :, None] == labels[None, None, :]
    onehot = jnp.sum(picked.astype(jnp.int32), axis=1)
    dense_gate = jnp.sum(jnp.where(picked, gates[:, :, None], zero_value), axis=1)
    slot_index = jnp.cumsum(onehot, axis=0) - onehot
    select = (slot_index.T[:, None, :] == places[None, :, None]) & (onehot.T[:, None, :] > 0)
    outgoing = jnp.einsum(
        "ect,td->ecd", select.astype(jnp.bfloat16), normed, preferred_element_type=jnp.float32
    ).astype(jnp.bfloat16)
    outgoing = outgoing.reshape(groups, local_experts, capacity, normed.shape[1])
    received = lax.all_to_all(outgoing, "ep", split_axis=0, concat_axis=0, tiled=True)
    results, shared_hidden = expert_apply(
        received, expert_gate, expert_up, expert_down, shared_gate_part, shared_up_part
    )
    returned = lax.all_to_all(results, "ep", split_axis=0, concat_axis=0, tiled=True)
    weight = jnp.where(select, dense_gate.T[:, None, :], zero_value)
    returned_rows = returned.reshape(experts_all, capacity, normed.shape[1]).astype(jnp.float32)
    routed = jnp.einsum("ect,ecd->td", weight, returned_rows, precision=lax.Precision.HIGHEST)
    shared_out = jnp.dot(shared_hidden, shared_down, preferred_element_type=jnp.float32)
    combined = routed + shared_out
    out_squares = lax.psum(jnp.sum(combined * combined, axis=1), "tp")
    return normalize(combined, out_gain, out_squares, D).astype(jnp.bfloat16)


F32 = jnp.float32
BF16 = jnp.bfloat16
LANES = 128


def flip(index, mask):
    out, bit = index, 1
    while bit <= mask:
        if mask & bit:
            out = out + bit - 2 * bit * ((index // bit) % 2)
        bit *= 2
    return out


def iota(shape, dim):
    return lax.broadcasted_iota(jnp.int32, shape, dim)


def dot(a, b):
    return jnp.dot(a, b, preferred_element_type=F32)


def batches(n_ep):
    far = list(range(2, n_ep, 2))
    return [[0], far[-2::-1], far[-1:]]


def fused_kernel(
    n_ep, n_tp, cap, width,
    tok_hbm, routes_hbm, gates_hbm, pre_hbm, eg_hbm, eu_hbm, ed_hbm, sg_hbm, su_hbm, sd_hbm, outg_hbm,
    o_ref,
    tok_ref, routes_ref, gates_ref, pre_ref, outg_ref,
    wg, wu, wd, sg, su, sd,
    xall, ss_all, bufs,
    rs_send, rs_recv, rsh_send, rsh_recv, rsh_own,
    hid_out, hid, hidsh, yown, yhold, ysend, ypair, zsend, zrecv, sq_all,
    w_sem, x_send, x_recv, ss_send, ss_recv, rs_ssem, rs_rsem, rsh_rsem,
    h_ssem, h_rsem, hs_rsem, p_ssem, p_rsem, y_rsem, q_ssem, q_rsem,
):
    me = lax.axis_index("ep")
    mine = lax.axis_index("tp")
    tok, dim = tok_ref.shape
    local = eg_hbm.shape[0]
    experts = local * n_ep
    top = routes_hbm.shape[0]
    part = eg_hbm.shape[2] // n_tp
    tp_masks = sorted(range(1, n_tp), key=lambda m: -bin(m).count("1"))
    evens = batches(n_ep)
    count = len(evens)
    order = [m for batch in evens for m in batch + [m + 1 for m in batch]]
    place = {m: i for i, m in enumerate(order)}
    owner = {m: b for b, batch in enumerate(evens) for m in batch}
    far = [m for batch in evens for m in batch if m]
    slot = {m: i for i, m in enumerate(far)}
    pairs = [len(batch) for batch in evens]
    start = [place[batch[0]] for batch in evens]
    span = [2 * p * tok for p in pairs]
    per = [2 * p * cap for p in pairs]
    rows = [local * p for p in per]

    def at_ep(mask):
        return {"ep": flip(me, mask)}

    def at_tp(mask):
        return {"tp": flip(mine, mask)}

    def across(mask):
        return {"ep": flip(me, 1), "tp": flip(mine, mask)}

    barrier = pltpu.get_barrier_semaphore()
    peers = [at_ep(m + 1) for m in [0] + far]
    peers += [where(m) for m in range(1, n_tp) for where in (at_tp, across)]
    for where in peers:
        pl.semaphore_signal(barrier, inc=1, device_id=where, device_id_type=pl.DeviceIdType.MESH)

    def columns(m):
        return pl.ds(pl.multiple_of(flip(mine, m) * part, part), part)

    copies = {}
    loads = (
        ("routes", routes_hbm, routes_ref), ("gates", gates_hbm, gates_ref), ("tok", tok_hbm, tok_ref),
        ("pre", pre_hbm, pre_ref),
    )
    for m in tp_masks + [0]:
        here = (slice(None), slice(None), columns(m))
        loads += ((("g", m), eg_hbm.at[here], wg.at[here]), (("u", m), eu_hbm.at[here], wu.at[here]))
    loads += (
        ("sg", sg_hbm, sg), ("su", su_hbm, su), ("sd", sd_hbm, sd), ("d", ed_hbm, wd), ("outg", outg_hbm, outg_ref),
    )
    for i, (name, src, dst) in enumerate(loads):
        copies[name] = pltpu.make_async_copy(src, dst, w_sem.at[i])
        if name not in ("sd", "d", "outg"):
            copies[name].start()

    def describe(src, dst, ssem, rsem, where):
        return pltpu.make_async_remote_copy(
            src_ref=src, dst_ref=dst, send_sem=ssem, recv_sem=rsem,
            device_id=where, device_id_type=pl.DeviceIdType.MESH,
        )

    def send(src, dst, ssem, rsem, where):
        describe(src, dst, ssem, rsem, where).start()

    def arrived(ref, ssem, rsem, where):
        describe(ref, ref, ssem, rsem, where).wait_recv()

    def sent(ref, ssem, rsem, where):
        describe(ref, ref, ssem, rsem, where).wait_send()

    def flat_gain(ref):
        value = ref[...].astype(F32)
        return jnp.concatenate([value[i : i + 1, :] for i in range(ref.shape[0])], axis=1)

    ss_all[:, 0] = jnp.zeros((ss_all.shape[0],) + ss_all.shape[2:], F32)
    for name in ("routes", "gates", "tok", "pre"):
        copies[name].wait()
    row = iota((LANES, tok), 0)
    names = row % experts
    dense = jnp.zeros((LANES, tok), F32)
    for k in range(top):
        dense = dense + jnp.where(routes_ref[k : k + 1, :] == names, gates_ref[k : k + 1, :], 0.0)
    named = jnp.where(dense > 0.0, 1.0, 0.0)

    def terms(value):
        hi = value.astype(BF16).astype(F32)
        mid = (value - hi).astype(BF16).astype(F32)
        return hi, mid, value - hi - mid

    def choose(index, values):
        out = 0.0
        for i, value in enumerate(values):
            out = jnp.where(index == i, value, out)
        return out

    def flipped(left, right):
        return lax.dot_general(
            jnp.where(left, 1.0, 0.0).astype(BF16), right.astype(BF16), (((1,), (1,)), ((), ())),
            preferred_element_type=F32,
        )

    here, there = iota((tok, tok), 0), iota((tok, tok), 1)
    meta = flipped(here == there, choose(row // experts, terms(dense) + (named,)))
    before = flipped(there < here, named)
    x = tok_ref[...].astype(F32)
    xall[0, :, :dim] = (x * flat_gain(pre_ref)).astype(BF16)
    squares = jnp.sum(x * x, axis=1, keepdims=True)
    lane = iota((tok, LANES), 1)
    meta = jnp.where(lane < 3 * experts, meta, meta * (before + 1.0))
    meta = jnp.where(lane < 4 * experts, meta, choose(lane - 4 * experts, terms(squares)))
    xall[0, :, dim:] = meta.astype(BF16)

    pl.semaphore_wait(barrier, len(peers))

    def x_to(m, held, put, index):
        send(xall.at[held], xall.at[put], x_send.at[0], x_recv.at[index], at_ep(m))

    odd = len(far)
    x_to(1, 0, place[1], odd)
    for m in far[-2::-1] + far[-1:]:
        x_to(m + 1, 0, place[m + 1], slot[m])

    def relay(m):
        arrived(xall.at[place[m + 1]], x_send.at[0], x_recv.at[slot[m]], at_ep(m + 1))
        x_to(1, place[m + 1], place[m], odd + owner[m])

    xs = xall[0, :, :dim]
    def shared_piece(m):
        g = dot(xs, sg[:, columns(m)])
        u = dot(xs, su[:, columns(m)])
        if m:
            rsh_send[m - 1, :, :part] = g.astype(BF16)
            rsh_send[m - 1, :, part:] = u.astype(BF16)
            send(rsh_send.at[m - 1], rsh_recv.at[m - 1], rs_ssem.at[0], rsh_rsem.at[0], at_tp(m))
        else:
            rsh_own[:, :part] = g
            rsh_own[:, part:] = u

    def from_pair(b):
        return xall.at[pl.ds(start[b] if b else place[1], pairs[b])]

    row8, lane8 = iota((8, LANES), 0), iota((8, LANES), 1)
    gate_lane = lane8 < 3 * experts
    slot_lane = (lane8 >= 3 * experts) & (lane8 < 4 * experts)
    mine8 = me * local + row8
    pair8 = flip(me, 1) * local + row8
    pick = (
        ((row8 < local) & gate_lane & (lane8 % experts == mine8))
        | ((row8 == local) & (lane8 >= 4 * experts))
        | ((row8 > local) & (row8 <= 2 * local) & slot_lane & (lane8 % experts == mine8 - local - 1))
        | ((row8 > 2 * local) & (row8 <= 3 * local) & slot_lane & (lane8 % experts == pair8 - 2 * local - 1))
    )
    pick = jnp.where(pick, 1.0, 0.0).astype(BF16)
    tables, chosen, others, scale, own = {}, {}, {}, {}, {}

    def gather(b):
        arrived(from_pair(b), x_send.at[0], x_recv.at[odd + b], at_ep(1))
        blocks = pl.ds(start[b], 2 * pairs[b])
        tail = xall[blocks, :, dim:].reshape(span[b], LANES)
        table = lax.dot_general(pick, tail, (((1,), (1,)), ((), ())), preferred_element_type=F32)
        ss_all[b, 0, :, : span[b]] = table[local : local + 1, :]
        for m in tp_masks:
            send(ss_all.at[b, 0], ss_all.at[b, m], ss_send.at[0], ss_recv.at[b], at_tp(m))
        block = iota((8, span[b]), 1) // tok
        seen = (block + pairs[b]) % (2 * pairs[b])
        block = jnp.where(iota((8, span[b]), 0) > 2 * local, seen, block)
        target = jnp.where(table > 0.5, block * cap - 1 + table.astype(jnp.int32), -rows[b])

        def piece_of(e, base):
            goal = target[base + e : base + e + 1, :] + e * per[b]
            return jnp.where(iota((rows[b], span[b]), 0) == goal, 1.0, 0.0)

        pieces = [piece_of(e, local + 1) for e in range(local)]
        others[b] = sum(piece_of(e, 2 * local + 1) for e in range(local))
        tables[b], chosen[b] = table, pieces
        flat = xall[blocks, :, :dim].reshape(span[b], dim)
        for e in range(local):
            bufs[b][e] = dot(pieces[e].astype(BF16), flat).astype(BF16)

    def piece(b, m):
        if b == 0:
            copies["g", m].wait()
            copies["u", m].wait()
        g, u = 0.0, 0.0
        for e in range(local):
            rhs = bufs[b][e]
            g = g + dot(rhs, wg[e, :, columns(m)])
            u = u + dot(rhs, wu[e, :, columns(m)])
        rs_send[b][m, :, :part] = g.astype(BF16)
        rs_send[b][m, :, part:] = u.astype(BF16)
        send(rs_send[b].at[m], rs_recv[b].at[m], rs_ssem.at[0], rs_rsem.at[b], across(m))

    def scales(b):
        arrived(ss_all.at[b, pl.ds(1, n_tp - 1)], ss_send.at[0], ss_recv.at[b], at_tp(1))
        ss = ss_all[b, 0, :, : span[b]]
        for m in range(1, n_tp):
            ss = ss + ss_all[b, m, :, : span[b]]
        scale[b] = lax.rsqrt(ss / width + 1e-06)

    def activate(sums, by):
        g, u = sums[:, :part] * by, sums[:, part:] * by
        return (g / (1.0 + jnp.exp(-g)) * u).astype(BF16)

    def hidden_at(b, m):
        return 1 + (b - 1) * n_tp + m if b else 0

    def act(b):
        by = jnp.sum(others[b] * scale[b], axis=1, keepdims=True)
        arrived(rs_recv[b], rs_ssem.at[0], rs_rsem.at[b], across(1))
        sums = rs_recv[b][0].astype(F32)
        for m in tp_masks:
            sums = sums + rs_recv[b][m].astype(F32)
        hid_out[b][...] = activate(sums, by)
        for m in tp_masks:
            send(hid_out[b], hid[b].at[m], h_ssem.at[0], h_rsem.at[hidden_at(b, m)], across(m))
        send(hid_out[b], hid[b].at[0], h_ssem.at[0], h_rsem.at[hidden_at(b, 0)], at_ep(1))

    def down(b, m, e, lo=0, hi=dim):
        depth = pl.ds(pl.multiple_of(flip(mine, m) * part, part), part)
        return dot(hid[b][m], wd[e, depth, lo:hi])

    def down_own(b):
        arrived(hid[b].at[0] if b else hid[b], h_ssem.at[0], h_rsem.at[hidden_at(b, 0)], at_ep(1))
        own[b] = [down(b, 0, e) for e in range(local)]

    def down_near(b):
        for m in tp_masks[1:]:
            if b:
                arrived(hid[b].at[m], h_ssem.at[0], h_rsem.at[hidden_at(b, m)], across(m))
            own[b] = [own[b][e] + down(b, m, e) for e in range(local)]

    def ypart(b):
        return pl.ds(start[b] // 2, pairs[b])

    def back(b, lo=0, hi=dim, index=0):
        m = tp_masks[0]
        if b and lo == 0:
            arrived(hid[b].at[m], h_ssem.at[0], h_rsem.at[hidden_at(b, m)], across(m))
        gated = 0.0
        for e in range(local):
            acc = own[b][e][:, lo:hi] + down(b, m, e, lo, hi)
            gated = gated + acc * jnp.sum(chosen[b][e] * tables[b][e : e + 1, :], axis=1, keepdims=True)
        y = lax.dot_general(
            sum(chosen[b]).astype(BF16), gated.astype(BF16), (((0,), (0,)), ((), ())), preferred_element_type=F32
        ).reshape(2 * pairs[b], tok, hi - lo)
        even, uneven = y[: pairs[b]], y[pairs[b] :]
        ysend[ypart(b), :, lo:hi] = (even if b else uneven).astype(BF16)
        yhold[ypart(b), :, lo:hi] = uneven if b else even
        block = (ypart(b), slice(None), pl.ds(lo, hi - lo))
        send(ysend.at[block], ypair.at[block], p_ssem.at[0], p_rsem.at[index], at_ep(1))

    def forward(b, lo=0, hi=dim, index=0):
        if b:
            block = (pl.ds(0, pairs[0] + pairs[1]) if b == 1 else ypart(b), slice(None), pl.ds(lo, hi - lo))
            arrived(ypair.at[block], p_ssem.at[0], p_rsem.at[index], at_ep(1))
        for i, m in enumerate(evens[b]):
            here = start[b] // 2 + i
            both = yhold[here, :, lo:hi] + ypair[here, :, lo:hi].astype(F32)
            if m:
                zsend[slot[m], :, lo:hi] = both.astype(BF16)
                block = (slot[m], slice(None), pl.ds(lo, hi - lo))
                send(zsend.at[block], zrecv.at[block], p_ssem.at[0], y_rsem.at[0], at_ep(m + 1))
            else:
                kept.append(both)

    def shared_act():
        match = jnp.where(iota((tok, span[0]), 1) == iota((tok, span[0]), 0), 1.0, 0.0)
        by = jnp.sum(match * scale[0], axis=1, keepdims=True)
        arrived(rsh_recv, rs_ssem.at[0], rsh_rsem.at[0], at_tp(1))
        sums = rsh_own[...]
        for m in tp_masks:
            sums = sums + rsh_recv[m - 1].astype(F32)
        hidsh[0] = activate(sums, by)
        for m in tp_masks:
            send(hidsh.at[0], hidsh.at[m], h_ssem.at[0], hs_rsem.at[0], at_tp(m))

    def shared_down():
        arrived(hidsh.at[pl.ds(1, n_tp - 1)], h_ssem.at[0], hs_rsem.at[0], at_tp(1))
        shared_out = 0.0
        for m in range(n_tp):
            depth = pl.ds(pl.multiple_of(flip(mine, m) * part, part), part)
            shared_out = shared_out + dot(hidsh[m], sd[depth, :])
        yown[...] = shared_out

    kept = []
    gather(0)
    for name in ("sd", "d", "outg"):
        copies[name].start()
    for m in tp_masks + [0]:
        piece(0, m)
    for m in evens[1]:
        relay(m)
    copies["sg"].wait()
    copies["su"].wait()
    for m in tp_masks + [0]:
        shared_piece(m)
    gather(1)
    piece(1, tp_masks[0])
    for m in evens[2]:
        relay(m)
    for m in tp_masks[1:]:
        piece(1, m)
    gather(2)
    for m in tp_masks:
        piece(2, m)
    scales(0)
    act(0)
    piece(1, 0)
    piece(2, 0)
    shared_act()
    copies["d"].wait()
    copies["sd"].wait()
    scales(1)
    act(1)
    scales(2)
    act(2)
    down_own(0)
    down_near(0)
    back(0)
    shared_down()
    down_own(1)
    down_own(2)
    down_near(1)
    back(1)
    down_near(2)
    back(2, 0, dim, 1)
    forward(1)
    forward(2, 0, dim, 1)
    forward(0)
    combined = yown[...]
    for both in kept:
        combined = combined + both
    copies["outg"].wait()
    arrived(zrecv, p_ssem.at[0], y_rsem.at[0], at_ep(3))
    for i in range(len(far)):
        combined = combined + zrecv[i].astype(F32)

    squared = combined * combined
    lanes = squared[:, :LANES]
    for c in range(LANES, dim, LANES):
        lanes = lanes + squared[:, c : c + LANES]
    sq_all[0] = lanes
    for m in tp_masks:
        send(sq_all.at[0], sq_all.at[m], q_ssem.at[0], q_rsem.at[0], at_tp(m))
    scaled = combined * flat_gain(outg_ref)
    arrived(sq_all.at[pl.ds(1, n_tp - 1)], q_ssem.at[0], q_rsem.at[0], at_tp(1))
    lanes = sq_all[0]
    for m in range(1, n_tp):
        lanes = lanes + sq_all[m]
    mean = jnp.sum(lanes, axis=1, keepdims=True) / width
    o_ref[...] = (scaled * lax.rsqrt(mean + 1e-06)).astype(BF16)
    sent(xall.at[pl.ds(0, n_ep - 1)], x_send.at[0], x_recv.at[0], at_ep(1))
    sent(ss_all.at[:, pl.ds(1, n_tp - 1)], ss_send.at[0], ss_recv.at[0], at_tp(1))
    lines = n_tp * sum(rows) + (n_tp - 1) * tok
    sent(wd.at[0, pl.ds(0, lines), pl.ds(0, 2 * part)], rs_ssem.at[0], rs_rsem.at[0], across(1))
    sent(wd.at[0, pl.ds(0, lines), pl.ds(0, part)], h_ssem.at[0], h_rsem.at[0], across(1))
    sent(wd.at[0, pl.ds(0, (sum(pairs) + len(far)) * tok), :], p_ssem.at[0], p_rsem.at[0], at_ep(1))
    sent(sq_all.at[pl.ds(1, n_tp - 1)], q_ssem.at[0], q_rsem.at[0], at_tp(1))


def fused(n_ep, n_tp, tokens, routes, gates, pre_gain, eg, eu, ed, sg, su, sd, out_gain):
    tok, dim = tokens.shape
    local, _, hidden = eg.shape
    top = routes.shape[1]
    cap = max(2, 3 * tok * top // (2 * local * n_ep))
    half = n_ep // 2
    evens = batches(n_ep)
    count = len(evens)
    rows = [local * 2 * len(batch) * cap for batch in evens]
    part = hidden // n_tp
    anywhere = pl.BlockSpec(memory_space=pl.ANY)
    sems = lambda n: pltpu.SemaphoreType.DMA((n,))
    return pl.pallas_call(
        functools.partial(fused_kernel, n_ep, n_tp, cap, dim * n_tp),
        out_shape=pltpu.VMEM((tok, dim), BF16),
        in_specs=[anywhere] * 11,
        out_specs=pl.BlockSpec(memory_space=pltpu.VMEM),
        scratch_shapes=[
            pltpu.VMEM((tok, dim), BF16), pltpu.VMEM((top, tok), jnp.int32), pltpu.VMEM((top, tok), F32),
            pltpu.VMEM((dim // LANES, LANES), BF16), pltpu.VMEM((dim // LANES, LANES), BF16),
            pltpu.VMEM(eg.shape, BF16), pltpu.VMEM(eu.shape, BF16), pltpu.VMEM(ed.shape, BF16),
            pltpu.VMEM(sg.shape, BF16), pltpu.VMEM(su.shape, BF16), pltpu.VMEM(sd.shape, BF16),
            pltpu.VMEM((n_ep, tok, dim + LANES), BF16),
            pltpu.VMEM((count, n_tp, 1, LANES), F32),
            [pltpu.VMEM((local, r, dim), BF16) for r in rows],
            [pltpu.VMEM((n_tp, r, 2 * part), BF16) for r in rows],
            [pltpu.VMEM((n_tp, r, 2 * part), BF16) for r in rows],
            pltpu.VMEM((n_tp - 1, tok, 2 * part), BF16),
            pltpu.VMEM((n_tp - 1, tok, 2 * part), BF16),
            pltpu.VMEM((tok, 2 * part), F32),
            [pltpu.VMEM((r, part), BF16) for r in rows],
            [pltpu.VMEM((n_tp, r, part), BF16) for r in rows],
            pltpu.VMEM((n_tp, tok, part), BF16),
            pltpu.VMEM((tok, dim), F32),
            pltpu.VMEM((half, tok, dim), F32),
            pltpu.VMEM((half, tok, dim), BF16),
            pltpu.VMEM((half, tok, dim), BF16),
            pltpu.VMEM((half - 1, tok, dim), BF16),
            pltpu.VMEM((half - 1, tok, dim), BF16),
            pltpu.VMEM((n_tp, tok, LANES), F32),
            sems(9 + 2 * n_tp),
            sems(1), sems(half - 1 + count), sems(1), sems(count), sems(1), sems(count), sems(1),
            sems(1), sems(1 + n_tp * (count - 1)), sems(1), sems(1), sems(2), sems(1), sems(1), sems(1),
        ],
        compiler_params=pltpu.CompilerParams(
            collective_id=0, has_side_effects=True, vmem_limit_bytes=60 * 1024 * 1024
        ),
    )(
        tokens, routes.T, gates.T, pre_gain.reshape(-1, LANES), eg, eu, ed, sg, su, sd,
        out_gain.reshape(-1, LANES),
    )


def fits(n_ep, n_tp, tokens, routes, eg):
    tok, dim = tokens.shape
    local, _, hidden = eg.shape
    experts = local * n_ep
    cap = max(2, 3 * tok * routes.shape[1] // (2 * experts))
    power = (n_ep & (n_ep - 1)) == 0 and (n_tp & (n_tp - 1)) == 0
    return (
        power
        and n_ep > 4
        and n_tp > 1
        and hidden % (LANES * n_tp) == 0
        and dim % LANES == 0
        and tok % 16 == 0
        and n_ep * tok == LANES
        and 4 * experts + 3 <= LANES
        and 3 * local < 8
    )


def per_device(*args):
    n_ep, n_tp = lax.axis_size("ep"), lax.axis_size("tp")
    if fits(n_ep, n_tp, args[0], args[1], args[4]):
        return fused(n_ep, n_tp, *args)
    return on_device(*args)


def solution(mesh):
    in_specs = (
        P("ep", "tp"),
        P("ep", None),
        P("ep", None),
        P("tp"),
        P("ep", "tp", None),
        P("ep", "tp", None),
        P("ep", None, "tp"),
        P("tp", None),
        P("tp", None),
        P(None, "tp"),
        P("tp"),
    )
    out_specs = P("ep", "tp")
    return jax.shard_map(
        per_device, mesh=mesh, in_specs=in_specs, out_specs=out_specs, check_vma=False
    )
```
